256 devices in a mesh: gr: 2 (over z_hi), fs: 16 (over z_lo, y), tp: 8 (over x, core).
Axes of the slice: x: 4, y: 4, z: 8 (z_hi: 2, z_lo: 4; z = z_hi * 4 + z_lo), core: 2. Of those that a mesh axis runs over, the one named last changes fastest.
Arguments:
- tokens: bfloat16 [8192, 2048], P(('gr', 'tp'), 'fs'), may hold values from -6 to 6
- routes: int32 [8192, 2], P(('gr', 'tp')), may hold values from 0 to 7, all different within a row; in each aligned block of 512 rows (0 to 511, 512 to 1023, ...) at most 192 rows name the same one
- route_weight: float32 [8192, 2], P(('gr', 'tp')), may hold values from 0.25 to 1
- norm_gain: float32 [2048], P(('gr', 'fs')), may hold values from 0.1 to 1.9
- gate_master: float32 [8, 2048, 2816], P(None, ('gr', 'fs'), 'tp'), may hold values from -0.125 to 0.125
- up_master: float32 [8, 2048, 2816], P(None, ('gr', 'fs'), 'tp'), may hold values from -0.125 to 0.125
- down_master: float32 [8, 2048, 2816], P(None, ('gr', 'fs'), 'tp'), may hold values from -0.109375 to 0.109375
Outputs:
- mixed_output: bfloat16 [8192, 2048], P(('gr', 'tp'), 'fs')
- gate_serving: bfloat16 [8, 2048, 2816], P('tp', None, 'fs')
- up_serving: bfloat16 [8, 2048, 2816], P('tp', None, 'fs')
- down_serving: bfloat16 [8, 2048, 2816], P('tp', None, 'fs')
The draws below stay inside these ranges and needn't reach their ends.
Inputs may be any that keep to these rules, and one draw needn't show every extreme that they name: `routes`: each row names two different experts. Within the rows of one block of 512 tokens (one index of gr+tp) no expert is named by more than 192 rows, and in some blocks one expert is named by exactly 192.
All inputs are finite; a program needn't handle non-finite values.
Results may differ from the reference program's by a relative error of at most 0.0082.
Values may be sent and summed in bfloat16 or wider, within the bound.
No kernel may reach another device: no remote copies, remote signals or barrier semaphores. Data moves between devices by JAX's collectives and lax.ppermute only.
A program may use at most 128 MiB of HBM per device.

```python
import math
import jax
import jax.numpy as jnp
import numpy as np
from jax import lax

D = 2048
EFF = 2816
EXPERTS = 8
TOK_DEV = 512
CAP = 192
TOKENS = 8192


def shard_levels(stream_key, dims, cuts, low, largest):
    loudness, own = 1.0, jax.random.fold_in(stream_key, 6)
    for dim, blocks in cuts:
        steps = jnp.exp(jax.random.uniform(jax.random.fold_in(own, dim), (blocks,), jnp.float32, low / len(cuts), largest / len(cuts)))
        loudness = loudness * jnp.repeat(steps, dims[dim] // blocks).reshape([-1 if axis == dim else 1 for axis in range(len(dims))])
    return loudness


def deal_out(stream_key, own, number, rows, count, top, bound, skew):
    ranking = jax.random.permutation(stream_key, count)
    heavy_load, common = portions_of(count, rows * top, bound, skew, True), portions_of(count, rows * top, bound, skew, False)
    places = jnp.arange(count)

    def named(tallies, rotation):
        used = int((tallies > 0).sum())
        fixed = max(1, used // 4)
        passed = fixed + (places - fixed + rotation * (used - fixed)) % max(1, count - fixed)
        return jnp.zeros((count,), jnp.int32).at[ranking[jnp.where(places < fixed, places, passed)]].set(jnp.asarray(tallies, jnp.int32))

    tallies = jnp.where(number % 4 == 0, named(heavy_load, number // 4), named(common, number - number // 4 - 1))
    mixed = jax.random.permutation(jax.random.fold_in(own, 3), count)
    source_of, sink = mixed[0:count // 2 * 2:2], mixed[1:count // 2 * 2:2]
    slack = jnp.minimum(tallies[source_of] - 1, bound - tallies[sink]) // 2
    slack = jnp.where((source_of == ranking[0]) | (sink == ranking[0]) | (tallies[sink] == 0), 0, jnp.maximum(slack, 0))
    passed = jax.random.randint(jax.random.fold_in(own, 4), (count // 2,), 0, 1 << 20) % (slack + 1)
    tallies = tallies.at[source_of].add(-passed).at[sink].add(passed)
    members = jnp.searchsorted(jnp.cumsum(tallies), jnp.arange(rows * top), side="right").astype(jnp.int32)
    grid = members.reshape(top, rows).T
    grid = grid[jax.random.permutation(jax.random.fold_in(own, 1), rows)]
    rotation = jax.random.randint(jax.random.fold_in(own, 2), (rows, 1), 0, top)
    return jnp.take_along_axis(grid, (jnp.arange(top)[None, :] + rotation) % top, axis=1)


def portions_of(count, total, reach, slope, full):
    portions = [(1 << 20) // math.isqrt(standing ** slope) + 1 for standing in range(1, count + 1)]
    largest = reach if full else min(reach, max(-(-total // count), total * portions[0] // sum(portions)))
    least = 1 if total - largest >= count - 1 else 0
    holding, rest = [largest] + [least] * (count - 1), total - largest - least * (count - 1)
    while rest > 0:
        candidates = [i for i in range(1, count) if holding[i] < largest] or [i for i in range(1, count) if holding[i] < reach]
        whole, left = sum([portions[i] for i in candidates]), rest
        for i in candidates:
            addition = min(reach - holding[i], max(1, left * portions[i] // whole), rest)
            holding[i] = holding[i] + addition
            rest = rest - addition
    return np.array(holding)


def normal_values(key, shape, deviation, bound, cuts=(), held_as=jnp.bfloat16):
    values = deviation * jax.random.normal(key, shape, jnp.float32)
    if cuts:
        values = values * shard_levels(key, shape, cuts, -0.22, 0.18)
    return jnp.clip(values, -bound, bound).astype(held_as)


def setup_inputs(seed: int = 0) -> dict:
    arg_keys = jax.random.split(jax.random.key(seed), 8)
    tokens = normal_values(arg_keys[0], (TOKENS, D), 1.0, 6.0, ((0, 16), (1, 16)))
    routes_keys = jax.random.split(jax.random.fold_in(arg_keys[1], 1), TOKENS // TOK_DEV)
    routes_turns = jax.random.permutation(jax.random.fold_in(arg_keys[1], 3), TOKENS // TOK_DEV)
    routes = jax.vmap(lambda own, number: deal_out(jax.random.fold_in(arg_keys[1], 2), own, number, TOK_DEV, EXPERTS, 2, CAP, 1))(routes_keys, routes_turns).reshape((TOKENS, 2))
    route_weight = jnp.clip(jnp.exp(math.log(1.0) - 1.3862944 * jax.random.uniform(arg_keys[2], (TOKENS, 2), jnp.float32) ** shard_levels(arg_keys[2], (TOKENS, 2), ((0, 16),), -0.2, 0.2)), 0.25, 1.0)
    norm_gain = jnp.clip(1.0 + 0.18 * jax.random.normal(arg_keys[3], (D,), jnp.float32), 0.1, 1.9)
    gate_master = normal_values(arg_keys[4], (EXPERTS, D, EFF), D ** -0.5, 0.125, ((1, 32), (2, 8)), jnp.float32)
    up_master = normal_values(arg_keys[5], (EXPERTS, D, EFF), D ** -0.5, 0.125, ((1, 32), (2, 8)), jnp.float32)
    down_master = normal_values(arg_keys[6], (EXPERTS, D, EFF), EFF ** -0.5, 0.109375, ((1, 32), (2, 8)), jnp.float32)
    return {"tokens": tokens, "routes": routes, "route_weight": route_weight, "norm_gain": norm_gain, "gate_master": gate_master, "up_master": up_master, "down_master": down_master}


norm_eps = 1e-06

def slot_table(routes, experts, capacity):
    flat_routes = routes.reshape(-1)
    onehot = (flat_routes[:, None] == jnp.arange(experts, dtype=jnp.int32)[None, :]).astype(jnp.int32)
    running = jnp.cumsum(onehot, axis=0)
    slot_index = lax.optimization_barrier(jnp.sum(onehot * (running - 1), axis=1))
    return (flat_routes * capacity + slot_index).astype(jnp.int32)

def reference(tokens, routes, route_weight, norm_gain, gate_master, up_master, down_master):
    gate_serving = (gate_master * norm_gain[None, :, None]).astype(jnp.bfloat16)
    up_serving = (up_master * norm_gain[None, :, None]).astype(jnp.bfloat16)
    down_serving = down_master.astype(jnp.bfloat16)
    blocks = TOKENS // TOK_DEV
    as_float = tokens.astype(jnp.float32)
    normed = (as_float * lax.rsqrt(lax.optimization_barrier(jnp.mean(as_float * as_float, axis=1, keepdims=True)) + norm_eps)).astype(jnp.bfloat16)
    normed = normed.reshape(blocks, TOK_DEV, D)
    route_blocks = routes.reshape(blocks, TOK_DEV, 2)

    def find_slots(block_routes):
        return slot_table(block_routes, EXPERTS, CAP)
    placing = jax.vmap(find_slots)(route_blocks)
    slot_rows = jnp.arange(EXPERTS * CAP, dtype=jnp.int32)

    def pick(block_places):
        return (slot_rows[:, None] == block_places[None, :]).reshape(EXPERTS * CAP, TOK_DEV, 2)

    def dispatch(block_places, block_rows):
        route_table = lax.optimization_barrier(jnp.sum(pick(block_places).astype(jnp.float32), axis=2)).astype(jnp.bfloat16)
        return jnp.dot(route_table, block_rows, preferred_element_type=jnp.float32).astype(jnp.bfloat16)
    outgoing = jax.vmap(dispatch)(placing, normed)
    outgoing = outgoing.reshape(blocks, EXPERTS, CAP, D).transpose(1, 0, 2, 3).reshape(EXPERTS, blocks * CAP, D)

    def expert(inputs):
        slots, w_gate, w_up, w_down = inputs
        gate_acc = jnp.dot(slots, w_gate, preferred_element_type=jnp.float32)
        up_acc = jnp.dot(slots, w_up, preferred_element_type=jnp.float32)
        hidden = (jax.nn.silu(gate_acc) * up_acc).astype(jnp.bfloat16)
        return lax.dot_general(hidden, w_down, (((1,), (1,)), ((), ())), preferred_element_type=jnp.float32)
    outputs = lax.map(expert, (outgoing, gate_serving, up_serving, down_serving))
    outputs = outputs.reshape(EXPERTS, blocks, CAP, D).transpose(1, 0, 2, 3).reshape(blocks, EXPERTS * CAP, D)

    def combine(block_places, weight, produced):
        weights = lax.optimization_barrier(jnp.sum(jnp.where(pick(block_places), weight.reshape(1, TOK_DEV, 2), 0.0), axis=2))
        return lax.dot_general(weights, produced, (((0,), (0,)), ((), ())), precision=lax.Precision.HIGHEST, preferred_element_type=jnp.float32)
    mixed_output = jax.vmap(combine)(placing, route_weight.reshape(blocks, TOK_DEV, 2), outputs)
    return (mixed_output.reshape(TOKENS, D).astype(jnp.bfloat16), gate_serving, up_serving, down_serving)
```

```python
import jax
import jax.numpy as jnp
from jax import lax
from jax.experimental import pallas as pl
from jax.experimental.pallas import tpu as pltpu
from jax.sharding import PartitionSpec as P


norm_eps = 1e-06
BF = jnp.bfloat16
F32 = jnp.float32
CAP, TOK, D, F = 192, 512, 2048, 176
MAIN, REM = 128, 48
PACK_GU, PACK_D = 176, 96
PACK = PACK_GU + PACK_D
NEAR, FAR = (0, 1), (4, 5, 2, 3, 6, 7)
TRIPS = ((1, 0, 576, FAR[:3]), (1, 1, 576, FAR[3:]), (0, 0, 384, NEAR))


def spec_vmem():
    return pl.BlockSpec(memory_space=pltpu.VMEM)


def call(body, outs, args, scratch=(), after=()):
    n, m = len(args), len(after)

    def run(*refs):
        body(*refs[:n], *refs[n + m :])

    return pl.pallas_call(
        run,
        out_shape=outs,
        in_specs=[pl.BlockSpec(memory_space=pltpu.SMEM)]
        + [spec_vmem()] * (n - 1)
        + [pl.BlockSpec(memory_space=pl.ANY)] * m,
        out_specs=jax.tree.map(lambda _: spec_vmem(), outs),
        scratch_shapes=list(scratch),
        compiler_params=pltpu.CompilerParams(vmem_limit_bytes=48 * 2**20),
    )(*args, *after)


def sds(*shape, dtype=BF):
    return jax.ShapeDtypeStruct(shape, dtype)


def peer(where, r):
    return ((where[0] + r // 2) % 4) * 2 + (where[1] + r % 2) % 2


def pack_body(where, gain, gate, up, down, *outs):
    g = gain[...]
    for r in range(8):
        e = peer(where, r)
        for top, mats in ((0, (gate[e] * g, up[e] * g)), (PACK_GU, (down[e],))):
            for h in range(2):
                pieces = []
                for m, mat in enumerate(mats):
                    at = top + 64 * m
                    outs[r][h, at : at + 64, :] = mat[:, h * F : h * F + MAIN].astype(BF)
                    rest = mat[:, h * F + MAIN : (h + 1) * F]
                    pieces += [rest[16 * i : 16 * i + 16] for i in range(4)]
                if len(mats) == 1:
                    pieces.append(jnp.zeros((16, 64), F32))
                row = jnp.concatenate(pieces, axis=1).astype(BF)
                for i in range(row.shape[1] // 128):
                    at = top + 64 * len(mats) + 16 * i
                    outs[r][h, at : at + 16, :] = row[:, 128 * i : 128 * i + 128]


def by_y_body(where, *refs):
    got, outs, held = refs[:8], refs[8:12], refs[12]
    for r in range(8):
        held[r] = got[r][...]
    x, c, z, y = where[0], where[1], where[2], where[3]
    for dy in range(4):
        to_y = (y + dy) % 4
        for k in range(4):
            dx = (x + 8 - z - k) % 4
            r = dx * 2 + (c + to_y // 2) % 2
            outs[dy][k] = held[r, to_y % 2]


def by_z_body(where, *refs):
    got, out = refs[:4], refs[4]
    for z8 in range(8):
        k = (z8 + 4 - where[2]) % 4
        for j in range(4):
            out[z8, j] = got[j][k]


def unpack_body(where, got, *outs):
    z, y = where[2], where[3]

    @pl.loop(0, 8)
    def _(z8):
        for j in range(4):
            block = z8 * 4 + (y + 4 - j) % 4
            at = pl.multiple_of(block * 64, 64)
            part = block // 2
            near = ((part // 4 + 4 - z) % 4) * 128 + (block % 2) * 64
            near = pl.multiple_of(near, 64)
            q = (part % 4 + 4 - y) % 4
            for top, mats in ((0, (0, 1)), (PACK_GU, (2,))):
                first = top + 64 * len(mats)
                row = jnp.concatenate(
                    [
                        got[z8, j, first + 16 * i : first + 16 * i + 16, :].astype(F32)
                        for i in range(3 if len(mats) == 2 else 2)
                    ],
                    axis=1,
                )
                for i, m in enumerate(mats):
                    main = got[z8, j, top + 64 * i : top + 64 * i + 64, :]
                    rest = jnp.concatenate(
                        [row[:, REM * p : REM * p + REM] for p in range(4 * i, 4 * i + 4)], axis=0
                    ).astype(BF)
                    outs[m][0, pl.ds(at, 64), 0:MAIN] = main
                    outs[m][0, pl.ds(at, 64), MAIN:F] = rest
                    outs[3 + m][q, pl.ds(near, 64), 0:MAIN] = main
                    outs[3 + m][q, pl.ds(near, 64), MAIN:F] = rest


def dispatch_body(where, routes, *refs):
    toks, outs, table, made = refs[:4], refs[4:12], refs[12], refs[13]
    r0, r1 = routes[0:1, :], routes[1:2, :]
    expert = lax.broadcasted_iota(jnp.int32, (8, TOK), 0)
    named = (r0 == expert) | (r1 == expert)
    before = (
        lax.broadcasted_iota(jnp.int32, (TOK, TOK), 0)
        < lax.broadcasted_iota(jnp.int32, (TOK, TOK), 1)
    ).astype(F32).astype(BF)
    count = jnp.dot(named.astype(F32).astype(BF), before, preferred_element_type=F32)
    table[...] = jnp.where(named, count, -1.0)
    x = jnp.concatenate([t[...] for t in toks], axis=1)
    slot = lax.broadcasted_iota(jnp.int32, (CAP, TOK), 0).astype(F32)

    @pl.loop(0, 8)
    def _(r):
        pick = (slot == table[pl.ds(peer(where, r), 1), :]).astype(F32).astype(BF)
        made[r] = jnp.dot(pick, x, preferred_element_type=F32).astype(BF)

    for r in range(8):
        outs[r][...] = made[r]


def rows_body(where, *refs):
    for i, ref in enumerate(refs[:-1]):
        refs[-1][CAP * i : CAP * i + CAP, :] = ref[...]


def ffn_body(where, *refs):
    xs, (wg, wu, wd), (own, plus, minus, keep) = refs[:4], refs[4:7], refs[7:]
    g = u = total = None
    for q in range(4):
        x = xs[q][...]
        xf = x.astype(F32)
        dg = jnp.dot(x, wg[q], preferred_element_type=F32)
        du = jnp.dot(x, wu[q], preferred_element_type=F32)
        s = xf * xf
        g, u, total = (dg, du, s) if g is None else (g + dg, u + du, total + s)
    scale = lax.rsqrt(jnp.sum(total, axis=1, keepdims=True) / D + norm_eps)
    g = g * scale
    u = u * scale
    hidden = (g / (1.0 + jnp.exp(-g)) * u).astype(BF)

    def out(q, half):
        w = wd[q, 256 * half : 256 * half + 256, :]
        return lax.dot_general(
            hidden, w, (((1,), (1,)), ((), ())), preferred_element_type=F32
        ).astype(BF)

    plus[:, 0:256] = out(2, 0)
    plus[:, 256:512] = out(1, 1)
    minus[:, 0:256] = out(3, 0)
    minus[:, 256:512] = out(2, 1)
    keep[:, 0:256] = out(1, 0)
    keep[:, 256:512] = out(3, 1)
    own[:, 0:256] = out(0, 0)
    own[:, 256:512] = out(0, 1)


def by_rows(body, where, tiled, whole, widths, n, block, after=()):
    tile = n // 2
    rows = lambda w, first=0: pl.BlockSpec((tile, w), lambda i: (i + first, 0))
    m = len(tiled) + len(whole) + 1

    def run(*refs):
        body(*refs[:m], *refs[m + len(after) :])

    return pl.pallas_call(
        run,
        grid=(2,),
        in_specs=[pl.BlockSpec(memory_space=pltpu.SMEM)]
        + [rows(a.shape[1], 2 * block) for a in tiled]
        + [pl.BlockSpec(a.shape, lambda i: (0, 0, 0)) for a in whole]
        + [pl.BlockSpec(memory_space=pl.ANY)] * len(after),
        out_specs=[rows(w) for w in widths],
        out_shape=[sds(n, w) for w in widths],
        compiler_params=pltpu.CompilerParams(vmem_limit_bytes=48 * 2**20),
    )(where, *tiled, *whole, *after)


def add_body(where, keep, from_left, from_right, out0, out1):
    out0[...] = (keep[:, 0:256].astype(F32) + from_left[:, 0:256].astype(F32)).astype(BF)
    out1[...] = (keep[:, 256:512].astype(F32) + from_right[:, 256:512].astype(F32)).astype(BF)


def sums_body(where, own, from_left, from_right, left, right, *outs):
    for i, out in enumerate(outs):
        at = slice(CAP * i, CAP * i + CAP)
        a = own[at, 0:256].astype(F32) + left[at, :].astype(F32)
        out[:, 0:256] = (a + from_right[at, 0:256].astype(F32)).astype(BF)
        b = own[at, 256:512].astype(F32) + right[at, :].astype(F32)
        out[:, 256:512] = (b + from_left[at, 256:512].astype(F32)).astype(BF)


def combine_body(relative, where, routes, weight, *refs):
    n = len(relative)
    got, outs, held = refs[:n], refs[n:-1], refs[-1]
    before_sum = None
    if len(outs) in (2, 5):
        before_sum, outs = outs[0], outs[1:]
    r0, r1 = routes[:, 0:1], routes[:, 1:2]
    w0, w1 = weight[:, 0:1], weight[:, 1:2]
    expert = lax.broadcasted_iota(jnp.int32, (TOK, 128), 1)
    one0, one1 = (r0 == expert).astype(F32), (r1 == expert).astype(F32)
    before = (
        lax.broadcasted_iota(jnp.int32, (TOK, TOK), 1)
        < lax.broadcasted_iota(jnp.int32, (TOK, TOK), 0)
    ).astype(F32).astype(BF)
    count = jnp.dot(before, (one0 + one1).astype(BF), preferred_element_type=F32)
    slot0 = jnp.sum(one0 * count, axis=1, keepdims=True)
    slot1 = jnp.sum(one1 * count, axis=1, keepdims=True)
    slot = lax.broadcasted_iota(jnp.int32, (TOK, CAP), 1).astype(F32)
    held[...] = jnp.zeros((TOK, 512), F32) if before_sum is None else before_sum[...]
    for i, r in enumerate(relative):
        e = peer(where, r)
        at = jnp.where(r0 == e, slot0, jnp.where(r1 == e, slot1, -1.0))
        w = jnp.where(r0 == e, w0, jnp.where(r1 == e, w1, 0.0))
        pick = (slot == at).astype(F32).astype(BF)
        held[...] += w * jnp.dot(pick, got[i][...], preferred_element_type=F32)
    if len(outs) == 1:
        outs[0][...] = held[...]
        return
    outs[0][...] = held[:, 0:128]
    for k in range(1, 4):
        outs[k][...] = held[:, 128 * k : 128 * k + 128].astype(BF)


def shift_tp(a, r, sign=1):
    dx, dc = sign * (r // 2), r % 2
    return lax.ppermute(
        a, "tp", [(2 * x + c, 2 * ((x + dx) % 4) + (c + dc) % 2) for x in range(4) for c in range(2)]
    )


def shift_fs(a, dz, dy):
    return lax.ppermute(
        a, "fs", [(4 * z + y, 4 * ((z + dz) % 4) + (y + dy) % 4) for z in range(4) for y in range(4)]
    )


def local(tokens, routes, route_weight, norm_gain, gate_master, up_master, down_master):
    tp, fs, gr = lax.axis_index("tp"), lax.axis_index("fs"), lax.axis_index("gr")
    where = jnp.stack([tp // 2, tp % 2, fs // 4, fs % 4, gr]).astype(jnp.int32)
    by_k = [tokens] * 4
    for k in (2, 1, 3):
        by_k[k] = shift_fs(tokens, -k, 0)
    packed = call(
        pack_body,
        [sds(2, PACK, 128)] * 8,
        (where, norm_gain[:, None], gate_master, up_master, down_master),
    )

    def over_tp(parts):
        out = list(parts)
        for r in (4, 5, 2, 3, 6, 7, 1):
            out[r] = shift_tp(parts[r], r)
        return out

    w_tp = over_tp(packed)
    slots = call(
        dispatch_body,
        [sds(CAP, 512)] * 8,
        (where, routes.T, *by_k),
        scratch=[pltpu.VMEM((8, TOK), F32), pltpu.VMEM((8, CAP, 512), BF)],
        after=(packed[0],),
    )
    at_expert = over_tp(slots)

    def gather_y(chunk, after):
        n = CAP * len(chunk)
        own = call(
            rows_body, [sds(n, 512)], (where, *(at_expert[r] for r in chunk)), after=after
        )[0]
        minus, plus, two = shift_fs(own, 0, -1), shift_fs(own, 0, 1), shift_fs(own, 0, 2)
        return own, minus, two, plus

    to_y = call(
        by_y_body,
        [sds(4, PACK, 128)] * 4,
        (where, *w_tp),
        scratch=[pltpu.VMEM((8, 2, PACK, 128), BF)],
        after=(slots[0],),
    )
    w_y = list(to_y)
    for dy in (2, 1, 3):
        w_y[dy] = shift_fs(to_y[dy], 0, dy)
    near = gather_y(NEAR, (to_y[0],))
    rows = (near, gather_y(FAR, (near[0],)))
    to_z = call(by_z_body, [sds(8, 4, PACK, 128)], (where, *w_y), after=(rows[1][0],))[0]
    w_z = lax.all_to_all(
        to_z,
        ("gr", "fs"),
        0,
        0,
        axis_index_groups=[[4 * z + y for z in range(8)] for y in range(4)],
        tiled=True,
    )
    gate_w, up_w, down_w, *ordered = call(
        unpack_body, [sds(1, D, F)] * 3 + [sds(4, 512, F)] * 3, (where, w_z)
    )
    made = []
    for i, block, n, _ in TRIPS:
        made.append(
            by_rows(
                ffn_body,
                where,
                rows[i],
                ordered,
                (512,) * 4,
                n,
                block,
                after=[m[0] for m in made[-1:]],
            )
        )

    def out_y(t):
        return shift_fs(made[t][1], 0, 1), shift_fs(made[t][2], 0, -1)

    def sum_y(t, got, after):
        n = TRIPS[t][2]
        sums = call(add_body, [sds(n, 256)] * 2, (where, made[t][3], *got), after=after)
        return sums[0], (shift_fs(sums[0], 0, 1), shift_fs(sums[1], 0, -1))

    def home(t, got, ends, after):
        places = TRIPS[t][3]
        sums = call(
            sums_body, [sds(CAP, 512)] * len(places), (where, made[t][0], *got, *ends), after=after
        )
        return sums[0], [p if r == 0 else shift_tp(p, r, -1) for r, p in zip(places, sums)]

    def combine(t, parts, before_sum, outs, after):
        return call(
            lambda *refs: combine_body(TRIPS[t][3], *refs),
            outs,
            (where, routes, route_weight, *parts, *before_sum),
            scratch=[pltpu.VMEM((TOK, 512), F32)],
            after=after,
        )

    got = [out_y(t) for t in range(3)]
    add0, ends0 = sum_y(0, got[0], (made[2][0],))
    add1, ends1 = sum_y(1, got[1], (add0,))
    sums0, home0 = home(0, got[0], ends0, (add1,))
    add2, ends2 = sum_y(2, got[2], (sums0,))
    sums1, home1 = home(1, got[1], ends1, (add2,))
    partial = [sds(TOK, 512, dtype=F32)]
    part0 = combine(0, home0, (), partial, (sums1,))
    sums2, home2 = home(2, got[2], ends2, (part0[0],))
    part1 = combine(1, home1, part0, partial, (sums2,))
    mixed = combine(2, home2, part1, [sds(TOK, 128, dtype=F32)] + [sds(TOK, 128)] * 3, ())
    out = mixed[0]
    for k in (2, 1, 3):
        got = shift_fs(mixed[k], k, 0)
        out = out + got.astype(F32)
    return (out.astype(BF), gate_w, up_w, down_w)


def solution(mesh):
    placed = (
        P(("gr", "tp"), "fs"),
        P(("gr", "tp"), None),
        P(("gr", "tp"), None),
        P(("gr", "fs")),
        P(None, ("gr", "fs"), "tp"),
        P(None, ("gr", "fs"), "tp"),
        P(None, ("gr", "fs"), "tp"),
    )

    return jax.shard_map(
        local,
        mesh=mesh,
        in_specs=placed,
        out_specs=(
            P(("gr", "tp"), "fs"),
            P("tp", None, "fs"),
            P("tp", None, "fs"),
            P("tp", None, "fs"),
        ),
        check_vma=False,
    )
```

```python
import jax
import jax.numpy as jnp
from jax import lax
from jax.experimental import pallas as pl
from jax.experimental.pallas import tpu as pltpu
from jax.sharding import PartitionSpec as P


norm_eps = 1e-06
BF = jnp.bfloat16
F32 = jnp.float32
CAP, TOK, D, F = 192, 512, 2048, 176
MAIN, REM = 128, 48
PACK_GU, PACK_D = 176, 96
PACK = PACK_GU + PACK_D
TRIPS = ((4, 5, 3, 7), (0, 1, 2, 6))
ROWS = CAP * 8
HALF = CAP * 4


def spec_vmem():
    return pl.BlockSpec(memory_space=pltpu.VMEM)


def call(body, outs, args, scratch=(), after=(), in_hbm=0):
    n, m = len(args), len(after)

    def run(*refs):
        body(*refs[:n], *refs[n + m :])

    return pl.pallas_call(
        run,
        out_shape=outs,
        in_specs=[pl.BlockSpec(memory_space=pltpu.SMEM)]
        + [spec_vmem()] * (n - 1 - in_hbm)
        + [pl.BlockSpec(memory_space=pltpu.HBM)] * in_hbm
        + [pl.BlockSpec(memory_space=pl.ANY)] * m,
        out_specs=jax.tree.map(lambda _: spec_vmem(), outs),
        scratch_shapes=list(scratch),
        compiler_params=pltpu.CompilerParams(vmem_limit_bytes=48 * 2**20),
    )(*args, *after)


def sds(*shape, dtype=BF):
    return jax.ShapeDtypeStruct(shape, dtype)


def peer(where, r):
    return ((where[0] + r // 2) % 4) * 2 + (where[1] + r % 2) % 2


def pack_body(where, gain, gate_hbm, up_hbm, down_hbm, *refs):
    outs, (gate, up, down, sems) = refs[:4], refs[4:]
    copies = [
        pltpu.make_async_copy(src, dst, sems.at[i])
        for i, (src, dst) in enumerate(((gate_hbm, gate), (up_hbm, up), (down_hbm, down)))
    ]
    for copy in copies:
        copy.start()
    g = gain[...]
    for copy in copies:
        copy.wait()
    for r in range(8):
        e = peer(where, r)
        for top, mats in ((0, (gate[e] * g, up[e] * g)), (PACK_GU, (down[e],))):
            for h in range(2):
                pieces = []
                for m, mat in enumerate(mats):
                    at = top + 64 * m
                    outs[r // 2][r % 2, h, at : at + 64, :] = mat[:, h * F : h * F + MAIN].astype(BF)
                    rest = mat[:, h * F + MAIN : (h + 1) * F]
                    pieces += [rest[16 * i : 16 * i + 16] for i in range(4)]
                if len(mats) == 1:
                    pieces.append(jnp.zeros((16, 64), F32))
                row = jnp.concatenate(pieces, axis=1).astype(BF)
                for i in range(row.shape[1] // 128):
                    at = top + 64 * len(mats) + 16 * i
                    outs[r // 2][r % 2, h, at : at + 16, :] = row[:, 128 * i : 128 * i + 128]


def swap_body(where, *refs):
    for dx in range(4):
        refs[4][dx] = refs[dx][1]


def by_y_body(where, *refs):
    got, swapped, outs, held = refs[:4], refs[4], refs[5:9], refs[9]
    for dx in range(4):
        held[2 * dx] = got[dx][0]
        held[2 * dx + 1] = swapped[dx]
    x, c, z, y = where[0], where[1], where[2], where[3]
    for dy in range(4):
        to_y = (y + dy) % 4
        for k in range(4):
            dx = (x + 8 - z - k) % 4
            r = dx * 2 + (c + to_y // 2) % 2
            outs[dy][k] = held[r, to_y % 2]


def by_z_body(where, *refs):
    got, out = refs[:4], refs[4]
    for z8 in range(8):
        k = (z8 + 4 - where[2]) % 4
        for j in range(4):
            out[z8, j] = got[j][k]


def unpack_body(where, got, *outs):
    z, y = where[2], where[3]

    @pl.loop(0, 8)
    def _(z8):
        for j in range(4):
            block = z8 * 4 + (y + 4 - j) % 4
            at = pl.multiple_of(block * 64, 64)
            part = block // 2
            near = ((part // 4 + 4 - z) % 4) * 128 + (block % 2) * 64
            near = pl.multiple_of(near, 64)
            q = (part % 4 + 4 - y) % 4
            for top, mats in ((0, (0, 1)), (PACK_GU, (2,))):
                first = top + 64 * len(mats)
                row = jnp.concatenate(
                    [
                        got[z8, j, first + 16 * i : first + 16 * i + 16, :].astype(F32)
                        for i in range(3 if len(mats) == 2 else 2)
                    ],
                    axis=1,
                )
                for i, m in enumerate(mats):
                    main = got[z8, j, top + 64 * i : top + 64 * i + 64, :]
                    rest = jnp.concatenate(
                        [row[:, REM * p : REM * p + REM] for p in range(4 * i, 4 * i + 4)], axis=0
                    ).astype(BF)
                    outs[m][0, pl.ds(at, 64), 0:MAIN] = main
                    outs[m][0, pl.ds(at, 64), MAIN:F] = rest
                    outs[3 + m][q, pl.ds(near, 64), 0:MAIN] = main
                    outs[3 + m][q, pl.ds(near, 64), MAIN:F] = rest


def dispatch_body(where, routes, *refs):
    toks, outs, table, made = refs[:4], refs[4:8], refs[8], refs[9]
    r0, r1 = routes[0:1, :], routes[1:2, :]
    expert = lax.broadcasted_iota(jnp.int32, (8, TOK), 0)
    named = (r0 == expert) | (r1 == expert)
    before = (
        lax.broadcasted_iota(jnp.int32, (TOK, TOK), 0)
        < lax.broadcasted_iota(jnp.int32, (TOK, TOK), 1)
    ).astype(F32).astype(BF)
    count = jnp.dot(named.astype(F32).astype(BF), before, preferred_element_type=F32)
    table[...] = jnp.where(named, count, -1.0)
    x = jnp.concatenate([t[...] for t in toks], axis=1)
    slot = lax.broadcasted_iota(jnp.int32, (CAP, TOK), 0).astype(F32)

    @pl.loop(0, 8)
    def _(r):
        pick = (slot == table[pl.ds(peer(where, r), 1), :]).astype(F32).astype(BF)
        made[r] = jnp.dot(pick, x, preferred_element_type=F32).astype(BF)

    for r in range(8):
        outs[r // 2][r % 2] = made[r]


def rows_body(where, *refs):
    got, swapped, out = refs[:4], refs[4], refs[5]
    for i, r in enumerate(TRIPS[0] + TRIPS[1]):
        part = swapped[r // 2] if r % 2 else got[r // 2][0]
        out[CAP * i : CAP * i + CAP, :] = part


def ffn_body(where, *refs):
    xs, (wg, wu, wd), (own, plus, minus, keep) = refs[:4], refs[4:7], refs[7:]
    g = u = total = None
    for q in range(4):
        x = xs[q][...]
        xf = x.astype(F32)
        dg = jnp.dot(x, wg[q], preferred_element_type=F32)
        du = jnp.dot(x, wu[q], preferred_element_type=F32)
        s = xf * xf
        g, u, total = (dg, du, s) if g is None else (g + dg, u + du, total + s)
    scale = lax.rsqrt(jnp.sum(total, axis=1, keepdims=True) / D + norm_eps)
    g = g * scale
    u = u * scale
    hidden = (g / (1.0 + jnp.exp(-g)) * u).astype(BF)

    def out(q, half):
        w = wd[q, 256 * half : 256 * half + 256, :]
        return lax.dot_general(
            hidden, w, (((1,), (1,)), ((), ())), preferred_element_type=F32
        ).astype(BF)

    plus[:, 0:256] = out(2, 0)
    plus[:, 256:512] = out(1, 1)
    minus[:, 0:256] = out(3, 0)
    minus[:, 256:512] = out(2, 1)
    keep[:, 0:256] = out(1, 0)
    keep[:, 256:512] = out(3, 1)
    own[:, 0:256] = out(0, 0)
    own[:, 256:512] = out(0, 1)


def by_rows(body, where, tiled, whole, widths, n, block, after=()):
    tile = n // 2
    rows = lambda w, first=0: pl.BlockSpec((tile, w), lambda i: (i + first, 0))
    m = len(tiled) + len(whole) + 1

    def run(*refs):
        body(*refs[:m], *refs[m + len(after) :])

    return pl.pallas_call(
        run,
        grid=(2,),
        in_specs=[pl.BlockSpec(memory_space=pltpu.SMEM)]
        + [rows(a.shape[1], 2 * block) for a in tiled]
        + [pl.BlockSpec(a.shape, lambda i: (0, 0, 0)) for a in whole]
        + [pl.BlockSpec(memory_space=pl.ANY)] * len(after),
        out_specs=[rows(w) for w in widths],
        out_shape=[sds(n, w) for w in widths],
        compiler_params=pltpu.CompilerParams(vmem_limit_bytes=48 * 2**20),
    )(where, *tiled, *whole, *after)


def add_body(where, keep, from_left, from_right, out0, out1):
    out0[...] = (keep[:, 0:256].astype(F32) + from_left[:, 0:256].astype(F32)).astype(BF)
    out1[...] = (keep[:, 256:512].astype(F32) + from_right[:, 256:512].astype(F32)).astype(BF)


def sums_body(where, own, from_left, from_right, left, right, *outs):
    for i, out in enumerate(outs):
        at = slice(CAP * i, CAP * i + CAP)
        a = own[at, 0:256].astype(F32) + left[at, :].astype(F32)
        out[:, 0:256] = (a + from_right[at, 0:256].astype(F32)).astype(BF)
        b = own[at, 256:512].astype(F32) + right[at, :].astype(F32)
        out[:, 256:512] = (b + from_left[at, 256:512].astype(F32)).astype(BF)


def plan_body(where, routes, weight, out):
    r0, r1 = routes[:, 0:1], routes[:, 1:2]
    w0, w1 = weight[:, 0:1], weight[:, 1:2]
    expert = lax.broadcasted_iota(jnp.int32, (TOK, 128), 1)
    one0, one1 = (r0 == expert).astype(F32), (r1 == expert).astype(F32)
    before = (
        lax.broadcasted_iota(jnp.int32, (TOK, TOK), 1)
        < lax.broadcasted_iota(jnp.int32, (TOK, TOK), 0)
    ).astype(F32).astype(BF)
    count = jnp.dot(before, (one0 + one1).astype(BF), preferred_element_type=F32)
    slot0 = jnp.sum(one0 * count, axis=1, keepdims=True)
    slot1 = jnp.sum(one1 * count, axis=1, keepdims=True)
    table = jnp.zeros((TOK, 128), F32)
    for r in range(8):
        e = peer(where, r)
        at = jnp.where(r0 == e, slot0, jnp.where(r1 == e, slot1, -1.0))
        w = jnp.where(r0 == e, w0, jnp.where(r1 == e, w1, 0.0))
        table = jnp.where(expert == r, at, jnp.where(expert == 8 + r, w, table))
    out[...] = table


def combine_body(relative, plan, *refs):
    n = len(relative)
    got, outs = refs[:n], refs[n:]
    slot = lax.broadcasted_iota(jnp.int32, (TOK, CAP), 1).astype(F32)
    total = None
    if len(outs) == 5:
        total, outs = outs[0][...], outs[1:]
    for i, r in enumerate(relative):
        pick = (slot == plan[:, r : r + 1]).astype(F32).astype(BF)
        part = plan[:, 8 + r : 9 + r] * jnp.dot(pick, got[i][...], preferred_element_type=F32)
        total = part if total is None else total + part
    if len(outs) == 1:
        outs[0][...] = total
        return
    outs[0][...] = total[:, 0:128]
    for k in range(1, 4):
        outs[k][...] = total[:, 128 * k : 128 * k + 128].astype(BF)


def shift_tp(a, r, sign=1):
    dx, dc = sign * (r // 2), r % 2
    return lax.ppermute(
        a, "tp", [(2 * x + c, 2 * ((x + dx) % 4) + (c + dc) % 2) for x in range(4) for c in range(2)]
    )


def shift_fs(a, dz, dy):
    return lax.ppermute(
        a, "fs", [(4 * z + y, 4 * ((z + dz) % 4) + (y + dy) % 4) for z in range(4) for y in range(4)]
    )


def local(tokens, routes, route_weight, norm_gain, gate_master, up_master, down_master):
    tp, fs, gr = lax.axis_index("tp"), lax.axis_index("fs"), lax.axis_index("gr")
    where = jnp.stack([tp // 2, tp % 2, fs // 4, fs % 4, gr]).astype(jnp.int32)
    by_k = [tokens] * 4
    for k in (2, 1, 3):
        by_k[k] = shift_fs(tokens, -k, 0)
    packed = call(
        pack_body,
        [sds(2, 2, PACK, 128)] * 4,
        (where, norm_gain[:, None], gate_master, up_master, down_master),
        scratch=[pltpu.VMEM(gate_master.shape, F32)] * 3 + [pltpu.SemaphoreType.DMA((3,))],
        in_hbm=3,
    )

    def over_x(parts):
        out = list(parts)
        for dx in (2, 1, 3):
            out[dx] = shift_tp(parts[dx], 2 * dx)
        return out

    def swap(parts, after):
        shape = (4, *parts[0].shape[1:])
        mine = call(swap_body, [sds(*shape)], (where, *parts), after=after)[0]
        return mine, shift_tp(mine, 1)

    w_x = over_x(packed)
    slots = call(
        dispatch_body,
        [sds(2, CAP, 512)] * 4,
        (where, routes.T, *by_k),
        scratch=[pltpu.VMEM((8, TOK), F32), pltpu.VMEM((8, CAP, 512), BF)],
        after=(packed[0],),
    )
    t_x = over_x(slots)
    _, w_core = swap(w_x, (slots[0],))

    to_y = call(
        by_y_body,
        [sds(4, PACK, 128)] * 4,
        (where, *w_x, w_core),
        scratch=[pltpu.VMEM((8, 2, PACK, 128), BF)],
    )
    w_y = list(to_y)
    for dy in (2, 1, 3):
        w_y[dy] = shift_fs(to_y[dy], 0, dy)
    plan = call(
        plan_body, [sds(TOK, 128, dtype=F32)], (where, routes, route_weight), after=(to_y[0],)
    )[0]
    _, t_core = swap(t_x, (plan,))
    own = call(rows_body, [sds(ROWS, 512)], (where, *t_x, t_core))[0]
    two, plus, minus = shift_fs(own, 0, 2), shift_fs(own, 0, 1), shift_fs(own, 0, -1)
    rows = (own, minus, two, plus)
    to_z = call(by_z_body, [sds(8, 4, PACK, 128)], (where, *w_y), after=(own,))[0]
    w_z = lax.all_to_all(
        to_z,
        ("gr", "fs"),
        0,
        0,
        axis_index_groups=[[4 * z + y for z in range(8)] for y in range(4)],
        tiled=True,
    )
    gate_w, up_w, down_w, *ordered = call(
        unpack_body, [sds(1, D, F)] * 3 + [sds(4, 512, F)] * 3, (where, w_z)
    )
    made = []
    for t in range(2):
        last = [m[0] for m in made[-1:]]
        made.append(by_rows(ffn_body, where, rows, ordered, (512,) * 4, HALF, t, after=last))

    def out_y(t):
        return shift_fs(made[t][1], 0, 1), shift_fs(made[t][2], 0, -1)

    def sum_y(t, got, after):
        sums = call(add_body, [sds(HALF, 256)] * 2, (where, made[t][3], *got), after=after)
        return sums[0], (shift_fs(sums[0], 0, 1), shift_fs(sums[1], 0, -1))

    def home(t, got, ends, after):
        places = TRIPS[t]
        sums = call(
            sums_body, [sds(CAP, 512)] * len(places), (where, made[t][0], *got, *ends), after=after
        )
        return sums[0], [p if r == 0 else shift_tp(p, r, -1) for r, p in zip(places, sums)]

    def combine(t, parts, outs, after=()):
        return call(
            lambda where, plan, *refs: combine_body(TRIPS[t], plan, *refs),
            outs,
            (where, plan, *parts),
            after=after,
        )

    got = [out_y(t) for t in range(2)]
    add0, ends0 = sum_y(0, got[0], (made[1][0],))
    add1, ends1 = sum_y(1, got[1], (add0,))
    sums0, home0 = home(0, got[0], ends0, (add1,))
    sums1, home1 = home(1, got[1], ends1, (sums0,))
    part = combine(0, home0, [sds(TOK, 512, dtype=F32)], (sums1,))
    mixed = combine(1, (*home1, *part), [sds(TOK, 128, dtype=F32)] + [sds(TOK, 128)] * 3)
    out = mixed[0]
    for k in (2, 1, 3):
        got = shift_fs(mixed[k], k, 0)
        out = out + got.astype(F32)
    return (out.astype(BF), gate_w, up_w, down_w)


def solution(mesh):
    placed = (
        P(("gr", "tp"), "fs"),
        P(("gr", "tp"), None),
        P(("gr", "tp"), None),
        P(("gr", "fs")),
        P(None, ("gr", "fs"), "tp"),
        P(None, ("gr", "fs"), "tp"),
        P(None, ("gr", "fs"), "tp"),
    )

    return jax.shard_map(
        local,
        mesh=mesh,
        in_specs=placed,
        out_specs=(
            P(("gr", "tp"), "fs"),
            P("tp", None, "fs"),
            P("tp", None, "fs"),
            P("tp", None, "fs"),
        ),
        check_vma=False,
    )
```

```python
import jax
import jax.numpy as jnp
from jax import lax
from jax.experimental import pallas as pl
from jax.experimental.pallas import tpu as pltpu
from jax.sharding import PartitionSpec as P


norm_eps = 1e-06
BF = jnp.bfloat16
F32 = jnp.float32
CAP, TOK, D, F = 192, 512, 2048, 176
MAIN, REM = 128, 48
PACK_GU, PACK_D = 176, 96
PACK = PACK_GU + PACK_D
TRIPS = ((4, 5), (3, 7, 2, 6, 1, 0))
ROWS = CAP * 8


def spec_vmem():
    return pl.BlockSpec(memory_space=pltpu.VMEM)


def call(body, outs, args, scratch=(), after=()):
    n, m = len(args), len(after)

    def run(*refs):
        body(*refs[:n], *refs[n + m :])

    return pl.pallas_call(
        run,
        out_shape=outs,
        in_specs=[pl.BlockSpec(memory_space=pltpu.SMEM)]
        + [spec_vmem()] * (n - 1)
        + [pl.BlockSpec(memory_space=pl.ANY)] * m,
        out_specs=jax.tree.map(lambda _: spec_vmem(), outs),
        scratch_shapes=list(scratch),
        compiler_params=pltpu.CompilerParams(vmem_limit_bytes=48 * 2**20),
    )(*args, *after)


def sds(*shape, dtype=BF):
    return jax.ShapeDtypeStruct(shape, dtype)


def peer(where, r):
    return ((where[0] + r // 2) % 4) * 2 + (where[1] + r % 2) % 2


def pack_body(where, gain, gate, up, down, *outs):
    g = gain[...]
    for r in range(8):
        e = peer(where, r)
        for top, mats in ((0, (gate[e] * g, up[e] * g)), (PACK_GU, (down[e],))):
            for h in range(2):
                pieces = []
                for m, mat in enumerate(mats):
                    at = top + 64 * m
                    outs[r // 2][r % 2, h, at : at + 64, :] = mat[:, h * F : h * F + MAIN].astype(BF)
                    rest = mat[:, h * F + MAIN : (h + 1) * F]
                    pieces += [rest[16 * i : 16 * i + 16] for i in range(4)]
                if len(mats) == 1:
                    pieces.append(jnp.zeros((16, 64), F32))
                row = jnp.concatenate(pieces, axis=1).astype(BF)
                for i in range(row.shape[1] // 128):
                    at = top + 64 * len(mats) + 16 * i
                    outs[r // 2][r % 2, h, at : at + 16, :] = row[:, 128 * i : 128 * i + 128]


def swap_body(where, *refs):
    for dx in range(4):
        refs[4][dx] = refs[dx][1]


def by_y_body(where, *refs):
    got, swapped, outs, held = refs[:4], refs[4], refs[5:9], refs[9]
    for dx in range(4):
        held[2 * dx] = got[dx][0]
        held[2 * dx + 1] = swapped[dx]
    x, c, z, y = where[0], where[1], where[2], where[3]
    for dy in range(4):
        to_y = (y + dy) % 4
        for k in range(4):
            dx = (x + 8 - z - k) % 4
            r = dx * 2 + (c + to_y // 2) % 2
            outs[dy][k] = held[r, to_y % 2]


def by_z_body(where, *refs):
    got, out = refs[:4], refs[4]
    for z8 in range(8):
        k = (z8 + 4 - where[2]) % 4
        for j in range(4):
            out[z8, j] = got[j][k]


def unpack_body(where, got, *outs):
    z, y = where[2], where[3]

    @pl.loop(0, 8)
    def _(z8):
        for j in range(4):
            block = z8 * 4 + (y + 4 - j) % 4
            part = block // 2
            near = ((part // 4 + 4 - z) % 4) * 128 + (block % 2) * 64
            near = pl.multiple_of(near, 64)
            q = (part % 4 + 4 - y) % 4
            for top, mats in ((0, (0, 1)), (PACK_GU, (2,))):
                first = top + 64 * len(mats)
                row = jnp.concatenate(
                    [
                        got[z8, j, first + 16 * i : first + 16 * i + 16, :].astype(F32)
                        for i in range(3 if len(mats) == 2 else 2)
                    ],
                    axis=1,
                )
                for i, m in enumerate(mats):
                    main = got[z8, j, top + 64 * i : top + 64 * i + 64, :]
                    rest = jnp.concatenate(
                        [row[:, REM * p : REM * p + REM] for p in range(4 * i, 4 * i + 4)], axis=0
                    ).astype(BF)
                    outs[m][q, pl.ds(near, 64), 0:MAIN] = main
                    outs[m][q, pl.ds(near, 64), MAIN:F] = rest


def serve_body(where, *refs):
    z, y = where[2], where[3]
    for m in range(3):
        for q in range(4):
            for k in range(4):
                at = pl.multiple_of((((z + k) % 4) * 4 + (y + q) % 4) * 128, 128)
                refs[3 + m][0, pl.ds(at, 128), :] = refs[m][q, 128 * k : 128 * k + 128, :]


def dispatch_body(where, table, *refs):
    toks, outs, made = refs[:4], refs[4:8], refs[8]
    x = jnp.concatenate([t[...] for t in toks], axis=1)
    slot = lax.broadcasted_iota(jnp.int32, (CAP, TOK), 0).astype(F32)

    @pl.loop(0, 8)
    def _(r):
        pick = (slot == table[pl.ds(peer(where, r), 1), :]).astype(F32).astype(BF)
        made[r] = jnp.dot(pick, x, preferred_element_type=F32).astype(BF)

    for r in range(8):
        outs[r // 2][r % 2] = made[r]


def rows_body(where, *refs):
    got, swapped, out = refs[:4], refs[4], refs[5]
    for i, r in enumerate(TRIPS[0] + TRIPS[1]):
        part = swapped[r // 2] if r % 2 else got[r // 2][0]
        out[CAP * i : CAP * i + CAP, :] = part


def ffn_body(where, *refs):
    xs, (wg, wu, wd), (own, plus, minus, keep) = refs[:4], refs[4:7], refs[7:]
    g = u = total = None
    for q in range(4):
        x = xs[q][...]
        xf = x.astype(F32)
        dg = jnp.dot(x, wg[q], preferred_element_type=F32)
        du = jnp.dot(x, wu[q], preferred_element_type=F32)
        s = xf * xf
        g, u, total = (dg, du, s) if g is None else (g + dg, u + du, total + s)
    scale = lax.rsqrt(jnp.sum(total, axis=1, keepdims=True) / D + norm_eps)
    g = g * scale
    u = u * scale
    hidden = (g / (1.0 + jnp.exp(-g)) * u).astype(BF)

    def out(q, half):
        w = wd[q, 256 * half : 256 * half + 256, :]
        return lax.dot_general(
            hidden, w, (((1,), (1,)), ((), ())), preferred_element_type=F32
        ).astype(BF)

    plus[:, 0:256] = out(2, 0)
    plus[:, 256:512] = out(1, 1)
    minus[:, 0:256] = out(3, 0)
    minus[:, 256:512] = out(2, 1)
    keep[:, 0:256] = out(1, 0)
    keep[:, 256:512] = out(3, 1)
    own[:, 0:256] = out(0, 0)
    own[:, 256:512] = out(0, 1)


def by_rows(body, where, tiled, whole, widths, n, first_tile, after=()):
    tile = 2 * CAP
    rows = lambda w, first=0: pl.BlockSpec((tile, w), lambda i: (i + first, 0))
    m = len(tiled) + len(whole) + 1

    def run(*refs):
        body(*refs[:m], *refs[m + len(after) :])

    return pl.pallas_call(
        run,
        grid=(n // tile,),
        in_specs=[pl.BlockSpec(memory_space=pltpu.SMEM)]
        + [rows(a.shape[1], first_tile) for a in tiled]
        + [pl.BlockSpec(a.shape, lambda i: (0, 0, 0)) for a in whole]
        + [pl.BlockSpec(memory_space=pl.ANY)] * len(after),
        out_specs=[rows(w) for w in widths],
        out_shape=[sds(n, w) for w in widths],
        compiler_params=pltpu.CompilerParams(vmem_limit_bytes=48 * 2**20),
    )(where, *tiled, *whole, *after)


def add_body(where, keep, from_left, from_right, out0, out1):
    out0[...] = (keep[:, 0:256].astype(F32) + from_left[:, 0:256].astype(F32)).astype(BF)
    out1[...] = (keep[:, 256:512].astype(F32) + from_right[:, 256:512].astype(F32)).astype(BF)


def sums_body(where, own, from_left, from_right, left, right, *outs):
    for i, out in enumerate(outs):
        at = slice(CAP * i, CAP * i + CAP)
        a = own[at, 0:256].astype(F32) + left[at, :].astype(F32)
        out[:, 0:256] = (a + from_right[at, 0:256].astype(F32)).astype(BF)
        b = own[at, 256:512].astype(F32) + right[at, :].astype(F32)
        out[:, 256:512] = (b + from_left[at, 256:512].astype(F32)).astype(BF)


def plan_body(where, routes, weight, routes_t, out, table_t):
    r0, r1 = routes[:, 0:1], routes[:, 1:2]
    w0, w1 = weight[:, 0:1], weight[:, 1:2]
    expert = lax.broadcasted_iota(jnp.int32, (TOK, 128), 1)
    one0, one1 = (r0 == expert).astype(F32), (r1 == expert).astype(F32)
    before = (
        lax.broadcasted_iota(jnp.int32, (TOK, TOK), 1)
        < lax.broadcasted_iota(jnp.int32, (TOK, TOK), 0)
    ).astype(F32).astype(BF)
    count = jnp.dot(before, (one0 + one1).astype(BF), preferred_element_type=F32)
    slot0 = jnp.sum(one0 * count, axis=1, keepdims=True)
    slot1 = jnp.sum(one1 * count, axis=1, keepdims=True)
    table = jnp.zeros((TOK, 128), F32)
    for r in range(8):
        e = peer(where, r)
        at = jnp.where(r0 == e, slot0, jnp.where(r1 == e, slot1, -1.0))
        w = jnp.where(r0 == e, w0, jnp.where(r1 == e, w1, 0.0))
        table = jnp.where(expert == r, at, jnp.where(expert == 8 + r, w, table))
    out[...] = table
    expert = lax.broadcasted_iota(jnp.int32, (8, TOK), 0)
    named = (routes_t[0:1, :] == expert) | (routes_t[1:2, :] == expert)
    before = (
        lax.broadcasted_iota(jnp.int32, (TOK, TOK), 0)
        < lax.broadcasted_iota(jnp.int32, (TOK, TOK), 1)
    ).astype(F32).astype(BF)
    count = jnp.dot(named.astype(F32).astype(BF), before, preferred_element_type=F32)
    table_t[...] = jnp.where(named, count, -1.0)


def combine_body(relative, plan, *refs):
    n = len(relative)
    got, outs = refs[:n], refs[n:]
    slot = lax.broadcasted_iota(jnp.int32, (TOK, CAP), 1).astype(F32)
    total = None
    if len(outs) == 5:
        total, outs = outs[0][...], outs[1:]
    for i, r in enumerate(relative):
        pick = (slot == plan[:, r : r + 1]).astype(F32).astype(BF)
        part = plan[:, 8 + r : 9 + r] * jnp.dot(pick, got[i][...], preferred_element_type=F32)
        total = part if total is None else total + part
    if len(outs) == 1:
        outs[0][...] = total
        return
    outs[0][...] = total[:, 0:128]
    for k in range(1, 4):
        outs[k][...] = total[:, 128 * k : 128 * k + 128].astype(BF)


def shift_tp(a, r, sign=1):
    dx, dc = sign * (r // 2), r % 2
    return lax.ppermute(
        a, "tp", [(2 * x + c, 2 * ((x + dx) % 4) + (c + dc) % 2) for x in range(4) for c in range(2)]
    )


def shift_fs(a, dz, dy):
    return lax.ppermute(
        a, "fs", [(4 * z + y, 4 * ((z + dz) % 4) + (y + dy) % 4) for z in range(4) for y in range(4)]
    )


def local(tokens, routes, route_weight, norm_gain, gate_master, up_master, down_master):
    tp, fs, gr = lax.axis_index("tp"), lax.axis_index("fs"), lax.axis_index("gr")
    where = jnp.stack([tp // 2, tp % 2, fs // 4, fs % 4, gr]).astype(jnp.int32)
    by_k = [tokens] * 4
    for k in (2, 1, 3):
        by_k[k] = shift_fs(tokens, -k, 0)
    plan, table = call(
        plan_body,
        [sds(TOK, 128, dtype=F32), sds(8, TOK, dtype=F32)],
        (where, routes, route_weight, routes.T),
    )
    packed = call(
        pack_body,
        [sds(2, 2, PACK, 128)] * 4,
        (where, norm_gain[:, None], gate_master, up_master, down_master),
        after=(plan,),
    )

    def over_x(parts):
        out = list(parts)
        for dx in (2, 1, 3):
            out[dx] = shift_tp(parts[dx], 2 * dx)
        return out

    def swap(parts, after):
        shape = (4, *parts[0].shape[1:])
        mine = call(swap_body, [sds(*shape)], (where, *parts), after=after)[0]
        return mine, shift_tp(mine, 1)

    w_x = over_x(packed)
    slots = call(
        dispatch_body,
        [sds(2, CAP, 512)] * 4,
        (where, table, *by_k),
        scratch=[pltpu.VMEM((8, CAP, 512), BF)],
        after=(packed[0],),
    )
    t_x = over_x(slots)
    _, w_core = swap(w_x, (slots[0],))

    to_y = call(
        by_y_body,
        [sds(4, PACK, 128)] * 4,
        (where, *w_x, w_core),
        scratch=[pltpu.VMEM((8, 2, PACK, 128), BF)],
    )
    w_y = list(to_y)
    for dy in (2, 1, 3):
        w_y[dy] = shift_fs(to_y[dy], 0, dy)
    _, t_core = swap(t_x, (to_y[0],))
    own = call(rows_body, [sds(ROWS, 512)], (where, *t_x, t_core))[0]
    two, plus, minus = shift_fs(own, 0, 2), shift_fs(own, 0, 1), shift_fs(own, 0, -1)
    rows = (own, minus, two, plus)
    to_z = call(by_z_body, [sds(8, 4, PACK, 128)], (where, *w_y), after=(own,))[0]
    w_z = lax.all_to_all(
        to_z,
        ("gr", "fs"),
        0,
        0,
        axis_index_groups=[[4 * z + y for z in range(8)] for y in range(4)],
        tiled=True,
    )
    ordered = call(unpack_body, [sds(4, 512, F)] * 3, (where, w_z))
    made = []
    for t in range(2):
        last = [m[0] for m in made[-1:]]
        n = CAP * len(TRIPS[t])
        made.append(by_rows(ffn_body, where, rows, ordered, (512,) * 4, n, t, after=last))

    def out_y(t):
        return shift_fs(made[t][1], 0, 1), shift_fs(made[t][2], 0, -1)

    def sum_y(t, got, after):
        n = CAP * len(TRIPS[t])
        sums = call(add_body, [sds(n, 256)] * 2, (where, made[t][3], *got), after=after)
        return sums[0], (shift_fs(sums[0], 0, 1), shift_fs(sums[1], 0, -1))

    def home(t, got, ends, after):
        places = TRIPS[t]
        sums = call(
            sums_body, [sds(CAP, 512)] * len(places), (where, made[t][0], *got, *ends), after=after
        )
        return sums[0], [p if r == 0 else shift_tp(p, r, -1) for r, p in zip(places, sums)]

    def combine(t, parts, outs, after=()):
        return call(
            lambda where, plan, *refs: combine_body(TRIPS[t], plan, *refs),
            outs,
            (where, plan, *parts),
            after=after,
        )

    got = [out_y(t) for t in range(2)]
    add0, ends0 = sum_y(0, got[0], (made[1][0],))
    gate_w, up_w, down_w = call(serve_body, [sds(1, D, F)] * 3, (where, *ordered), after=(add0,))
    add1, ends1 = sum_y(1, got[1], (gate_w,))
    sums0, home0 = home(0, got[0], ends0, (add1,))
    sums1, home1 = home(1, got[1], ends1, (sums0,))
    part = combine(0, home0, [sds(TOK, 512, dtype=F32)], (sums1,))
    mixed = combine(1, (*home1, *part), [sds(TOK, 128, dtype=F32)] + [sds(TOK, 128)] * 3)
    out = mixed[0]
    for k in (2, 1, 3):
        got = shift_fs(mixed[k], k, 0)
        out = out + got.astype(F32)
    return (out.astype(BF), gate_w, up_w, down_w)


def solution(mesh):
    placed = (
        P(("gr", "tp"), "fs"),
        P(("gr", "tp"), None),
        P(("gr", "tp"), None),
        P(("gr", "fs")),
        P(None, ("gr", "fs"), "tp"),
        P(None, ("gr", "fs"), "tp"),
        P(None, ("gr", "fs"), "tp"),
    )

    return jax.shard_map(
        local,
        mesh=mesh,
        in_specs=placed,
        out_specs=(
            P(("gr", "tp"), "fs"),
            P("tp", None, "fs"),
            P("tp", None, "fs"),
            P("tp", None, "fs"),
        ),
        check_vma=False,
    )
```

```python
import jax
import jax.numpy as jnp
from jax import lax
from jax.experimental import pallas as pl
from jax.experimental.pallas import tpu as pltpu
from jax.sharding import PartitionSpec as P


norm_eps = 1e-06
BF = jnp.bfloat16
F32 = jnp.float32
CAP, TOK, D, F = 192, 512, 2048, 176
MAIN, REM = 128, 48
PACK_GU, PACK_D = 176, 88
PACK = PACK_GU + PACK_D
TRIPS = ((4, 5), (3, 7, 2, 6, 1, 0))
ROWS = CAP * 8


def spec_vmem():
    return pl.BlockSpec(memory_space=pltpu.VMEM)


def call(body, outs, args, scratch=(), after=()):
    n, m = len(args), len(after)

    def run(*refs):
        body(*refs[:n], *refs[n + m :])

    return pl.pallas_call(
        run,
        out_shape=outs,
        in_specs=[pl.BlockSpec(memory_space=pltpu.SMEM)]
        + [spec_vmem()] * (n - 1)
        + [pl.BlockSpec(memory_space=pl.ANY)] * m,
        out_specs=jax.tree.map(lambda _: spec_vmem(), outs),
        scratch_shapes=list(scratch),
        compiler_params=pltpu.CompilerParams(vmem_limit_bytes=48 * 2**20),
    )(*args, *after)


def sds(*shape, dtype=BF):
    return jax.ShapeDtypeStruct(shape, dtype)


def peer(where, r):
    return ((where[0] + r // 2) % 4) * 2 + (where[1] + r % 2) % 2


def pack_body(where, gain, gate, up, down, *outs):
    g = gain[...]
    for r in range(8):
        e = peer(where, r)
        for top, mats in ((0, (gate[e] * g, up[e] * g)), (PACK_GU, (down[e],))):
            for h in range(2):
                pieces = []
                for m, mat in enumerate(mats):
                    at = top + 64 * m
                    outs[r // 2][r % 2, h, at : at + 64, :] = mat[:, h * F : h * F + MAIN].astype(BF)
                    rest = mat[:, h * F + MAIN : (h + 1) * F]
                    pieces += [rest[8 * i : 8 * i + 8] for i in range(8)]
                row = jnp.concatenate(pieces, axis=1)
                at = top + 64 * len(mats)
                rest = [row[:, 128 * i : 128 * i + 128] for i in range(row.shape[1] // 128)]
                outs[r // 2][r % 2, h, at : at + 8 * len(rest), :] = jnp.concatenate(
                    rest, axis=0
                ).astype(BF)


def swap_body(where, *refs):
    for dx in range(4):
        refs[4][dx] = refs[dx][1]


def by_y_body(where, *refs):
    got, swapped, outs, held = refs[:4], refs[4], refs[5:9], refs[9]
    for dx in range(4):
        held[2 * dx] = got[dx][0]
        held[2 * dx + 1] = swapped[dx]
    x, c, z, y = where[0], where[1], where[2], where[3]
    for dy in range(4):
        to_y = (y + dy) % 4
        for k in range(4):
            dx = (x + 8 - z - k) % 4
            r = dx * 2 + (c + to_y // 2) % 2
            outs[dy][k] = held[r, to_y % 2]


def by_z_body(where, *refs):
    got, out = refs[:4], refs[4]
    for z8 in range(8):
        k = (z8 + 4 - where[2]) % 4
        for j in range(4):
            out[z8, j] = got[j][k]


def unpack_body(where, got, *outs):
    z, y = where[2], where[3]

    @pl.loop(0, 8)
    def _(z8):
        for j in range(4):
            block = z8 * 4 + (y + 4 - j) % 4
            part = block // 2
            near = ((part // 4 + 4 - z) % 4) * 128 + (block % 2) * 64
            near = pl.multiple_of(near, 64)
            q = (part % 4 + 4 - y) % 4
            for top, mats in ((0, (0, 1)), (PACK_GU, (2,))):
                first, tiles = top + 64 * len(mats), 3 * len(mats)
                flat = got[z8, j, first : first + 8 * tiles, :].astype(F32)
                row = jnp.concatenate([flat[8 * i : 8 * i + 8] for i in range(tiles)], axis=1)
                for i, m in enumerate(mats):
                    main = got[z8, j, top + 64 * i : top + 64 * i + 64, :]
                    rest = jnp.concatenate(
                        [row[:, REM * p : REM * p + REM] for p in range(8 * i, 8 * i + 8)], axis=0
                    ).astype(BF)
                    outs[m][q, pl.ds(near, 64), 0:MAIN] = main
                    outs[m][q, pl.ds(near, 64), MAIN:F] = rest


def serve_body(where, *refs):
    z, y = where[2], where[3]
    for m in range(3):
        for q in range(4):
            for k in range(4):
                at = pl.multiple_of((((z + k) % 4) * 4 + (y + q) % 4) * 128, 128)
                refs[3 + m][0, pl.ds(at, 128), :] = refs[m][q, 128 * k : 128 * k + 128, :]


def dispatch_body(where, routes, *refs):
    toks, outs, table, made = refs[:4], refs[4:8], refs[8], refs[9]
    expert = lax.broadcasted_iota(jnp.int32, (8, TOK), 0)
    named = (routes[0:1, :] == expert) | (routes[1:2, :] == expert)
    before = (
        lax.broadcasted_iota(jnp.int32, (TOK, TOK), 0)
        < lax.broadcasted_iota(jnp.int32, (TOK, TOK), 1)
    ).astype(F32).astype(BF)
    count = jnp.dot(named.astype(F32).astype(BF), before, preferred_element_type=F32)
    table[...] = jnp.where(named, count, -1.0)
    x = jnp.concatenate([t[...] for t in toks], axis=1)
    slot = lax.broadcasted_iota(jnp.int32, (CAP, TOK), 0).astype(F32)

    @pl.loop(0, 8)
    def _(r):
        pick = (slot == table[pl.ds(peer(where, r), 1), :]).astype(F32).astype(BF)
        made[r] = jnp.dot(pick, x, preferred_element_type=F32).astype(BF)

    for r in range(8):
        outs[r // 2][r % 2] = made[r]


def rows_body(where, *refs):
    got, swapped, out = refs[:4], refs[4], refs[5]
    for i, r in enumerate(TRIPS[0] + TRIPS[1]):
        part = swapped[r // 2] if r % 2 else got[r // 2][0]
        out[CAP * i : CAP * i + CAP, :] = part


def ffn_body(where, *refs):
    xs, (wg, wu, wd), (own, plus, minus, keep) = refs[:4], refs[4:7], refs[7:]
    g = u = total = None
    for q in range(4):
        x = xs[q][...]
        xf = x.astype(F32)
        dg = jnp.dot(x, wg[q], preferred_element_type=F32)
        du = jnp.dot(x, wu[q], preferred_element_type=F32)
        s = xf * xf
        g, u, total = (dg, du, s) if g is None else (g + dg, u + du, total + s)
    scale = lax.rsqrt(jnp.sum(total, axis=1, keepdims=True) / D + norm_eps)
    g = g * scale
    u = u * scale
    hidden = (g / (1.0 + jnp.exp(-g)) * u).astype(BF)

    def out(q, half):
        w = wd[q, 256 * half : 256 * half + 256, :]
        return lax.dot_general(
            hidden, w, (((1,), (1,)), ((), ())), preferred_element_type=F32
        ).astype(BF)

    plus[:, 0:256] = out(2, 0)
    plus[:, 256:512] = out(1, 1)
    minus[:, 0:256] = out(3, 0)
    minus[:, 256:512] = out(2, 1)
    keep[:, 0:256] = out(1, 0)
    keep[:, 256:512] = out(3, 1)
    own[:, 0:256] = out(0, 0)
    own[:, 256:512] = out(0, 1)


def by_rows(body, where, tiled, whole, widths, n, first_tile, after=()):
    tile = 2 * CAP
    rows = lambda w, first=0: pl.BlockSpec((tile, w), lambda i: (i + first, 0))
    m = len(tiled) + len(whole) + 1

    def run(*refs):
        body(*refs[:m], *refs[m + len(after) :])

    return pl.pallas_call(
        run,
        grid=(n // tile,),
        in_specs=[pl.BlockSpec(memory_space=pltpu.SMEM)]
        + [rows(a.shape[1], first_tile) for a in tiled]
        + [pl.BlockSpec(a.shape, lambda i: (0, 0, 0)) for a in whole]
        + [pl.BlockSpec(memory_space=pl.ANY)] * len(after),
        out_specs=[rows(w) for w in widths],
        out_shape=[sds(n, w) for w in widths],
        compiler_params=pltpu.CompilerParams(vmem_limit_bytes=48 * 2**20),
    )(where, *tiled, *whole, *after)


def add_body(where, keep, from_left, from_right, out0, out1):
    out0[...] = (keep[:, 0:256].astype(F32) + from_left[:, 0:256].astype(F32)).astype(BF)
    out1[...] = (keep[:, 256:512].astype(F32) + from_right[:, 256:512].astype(F32)).astype(BF)


def sums_body(where, own, from_left, from_right, left, right, *outs):
    for i, out in enumerate(outs):
        at = slice(CAP * i, CAP * i + CAP)
        a = own[at, 0:256].astype(F32) + left[at, :].astype(F32)
        out[:, 0:256] = (a + from_right[at, 0:256].astype(F32)).astype(BF)
        b = own[at, 256:512].astype(F32) + right[at, :].astype(F32)
        out[:, 256:512] = (b + from_left[at, 256:512].astype(F32)).astype(BF)


def plan_body(where, routes, weight, out):
    r0, r1 = routes[:, 0:1], routes[:, 1:2]
    w0, w1 = weight[:, 0:1], weight[:, 1:2]
    expert = lax.broadcasted_iota(jnp.int32, (TOK, 128), 1)
    one0, one1 = (r0 == expert).astype(F32), (r1 == expert).astype(F32)
    before = (
        lax.broadcasted_iota(jnp.int32, (TOK, TOK), 1)
        < lax.broadcasted_iota(jnp.int32, (TOK, TOK), 0)
    ).astype(F32).astype(BF)
    count = jnp.dot(before, (one0 + one1).astype(BF), preferred_element_type=F32)
    slot0 = jnp.sum(one0 * count, axis=1, keepdims=True)
    slot1 = jnp.sum(one1 * count, axis=1, keepdims=True)
    table = jnp.zeros((TOK, 128), F32)
    for r in range(8):
        e = peer(where, r)
        at = jnp.where(r0 == e, slot0, jnp.where(r1 == e, slot1, -1.0))
        w = jnp.where(r0 == e, w0, jnp.where(r1 == e, w1, 0.0))
        table = jnp.where(expert == r, at, jnp.where(expert == 8 + r, w, table))
    out[...] = table


def combine_body(relative, plan, *refs):
    n = len(relative)
    got, outs = refs[:n], refs[n:]
    slot = lax.broadcasted_iota(jnp.int32, (TOK, CAP), 1).astype(F32)
    total = None
    if len(outs) == 5:
        total, outs = outs[0][...], outs[1:]
    for i, r in enumerate(relative):
        pick = (slot == plan[:, r : r + 1]).astype(F32).astype(BF)
        part = plan[:, 8 + r : 9 + r] * jnp.dot(pick, got[i][...], preferred_element_type=F32)
        total = part if total is None else total + part
    if len(outs) == 1:
        outs[0][...] = total
        return
    outs[0][...] = total[:, 0:128]
    for k in range(1, 4):
        outs[k][...] = total[:, 128 * k : 128 * k + 128].astype(BF)


def shift_tp(a, r, sign=1):
    dx, dc = sign * (r // 2), r % 2
    return lax.ppermute(
        a, "tp", [(2 * x + c, 2 * ((x + dx) % 4) + (c + dc) % 2) for x in range(4) for c in range(2)]
    )


def shift_fs(a, dz, dy):
    return lax.ppermute(
        a, "fs", [(4 * z + y, 4 * ((z + dz) % 4) + (y + dy) % 4) for z in range(4) for y in range(4)]
    )


def local(tokens, routes, route_weight, norm_gain, gate_master, up_master, down_master):
    tp, fs, gr = lax.axis_index("tp"), lax.axis_index("fs"), lax.axis_index("gr")
    where = jnp.stack([tp // 2, tp % 2, fs // 4, fs % 4, gr]).astype(jnp.int32)
    by_k = [tokens] * 4
    for k in (2, 1, 3):
        by_k[k] = shift_fs(tokens, -k, 0)
    packed = call(
        pack_body,
        [sds(2, 2, PACK, 128)] * 4,
        (where, norm_gain[:, None], gate_master, up_master, down_master),
    )

    def over_x(parts):
        out = list(parts)
        for dx in (2, 1, 3):
            out[dx] = shift_tp(parts[dx], 2 * dx)
        return out

    def swap(parts, after):
        shape = (4, *parts[0].shape[1:])
        mine = call(swap_body, [sds(*shape)], (where, *parts), after=after)[0]
        return mine, shift_tp(mine, 1)

    w_x = over_x(packed)
    slots = call(
        dispatch_body,
        [sds(2, CAP, 512)] * 4,
        (where, routes.T, *by_k),
        scratch=[pltpu.VMEM((8, TOK), F32), pltpu.VMEM((8, CAP, 512), BF)],
        after=(packed[0],),
    )
    t_x = over_x(slots)
    _, w_core = swap(w_x, (slots[0],))

    to_y = call(
        by_y_body,
        [sds(4, PACK, 128)] * 4,
        (where, *w_x, w_core),
        scratch=[pltpu.VMEM((8, 2, PACK, 128), BF)],
    )
    w_y = list(to_y)
    for dy in (2, 1, 3):
        w_y[dy] = shift_fs(to_y[dy], 0, dy)
    plan = call(
        plan_body, [sds(TOK, 128, dtype=F32)], (where, routes, route_weight), after=(to_y[0],)
    )[0]
    _, t_core = swap(t_x, (plan,))
    own = call(rows_body, [sds(ROWS, 512)], (where, *t_x, t_core))[0]
    two, plus, minus = shift_fs(own, 0, 2), shift_fs(own, 0, 1), shift_fs(own, 0, -1)
    rows = (own, minus, two, plus)
    to_z = call(by_z_body, [sds(8, 4, PACK, 128)], (where, *w_y), after=(own,))[0]
    w_z = lax.all_to_all(
        to_z,
        ("gr", "fs"),
        0,
        0,
        axis_index_groups=[[4 * z + y for z in range(8)] for y in range(4)],
        tiled=True,
    )
    ordered = call(unpack_body, [sds(4, 512, F)] * 3, (where, w_z))
    made = []
    for t in range(2):
        last = [m[0] for m in made[-1:]]
        n = CAP * len(TRIPS[t])
        made.append(by_rows(ffn_body, where, rows, ordered, (512,) * 4, n, t, after=last))

    def out_y(t):
        return shift_fs(made[t][1], 0, 1), shift_fs(made[t][2], 0, -1)

    def sum_y(t, got, after):
        n = CAP * len(TRIPS[t])
        sums = call(add_body, [sds(n, 256)] * 2, (where, made[t][3], *got), after=after)
        return sums[0], (shift_fs(sums[0], 0, 1), shift_fs(sums[1], 0, -1))

    def home(t, got, ends, after):
        places = TRIPS[t]
        sums = call(
            sums_body, [sds(CAP, 512)] * len(places), (where, made[t][0], *got, *ends), after=after
        )
        return sums[0], [p if r == 0 else shift_tp(p, r, -1) for r, p in zip(places, sums)]

    def combine(t, parts, outs, after=()):
        return call(
            lambda where, plan, *refs: combine_body(TRIPS[t], plan, *refs),
            outs,
            (where, plan, *parts),
            after=after,
        )

    got = [out_y(t) for t in range(2)]
    add0, ends0 = sum_y(0, got[0], (made[1][0],))
    gate_w, up_w, down_w = call(serve_body, [sds(1, D, F)] * 3, (where, *ordered), after=(add0,))
    add1, ends1 = sum_y(1, got[1], (gate_w,))
    sums0, home0 = home(0, got[0], ends0, (add1,))
    sums1, home1 = home(1, got[1], ends1, (sums0,))
    part = combine(0, home0, [sds(TOK, 512, dtype=F32)], (sums1,))
    mixed = combine(1, (*home1, *part), [sds(TOK, 128, dtype=F32)] + [sds(TOK, 128)] * 3)
    out = mixed[0]
    for k in (2, 1, 3):
        got = shift_fs(mixed[k], k, 0)
        out = out + got.astype(F32)
    return (out.astype(BF), gate_w, up_w, down_w)


def solution(mesh):
    placed = (
        P(("gr", "tp"), "fs"),
        P(("gr", "tp"), None),
        P(("gr", "tp"), None),
        P(("gr", "fs")),
        P(None, ("gr", "fs"), "tp"),
        P(None, ("gr", "fs"), "tp"),
        P(None, ("gr", "fs"), "tp"),
    )

    return jax.shard_map(
        local,
        mesh=mesh,
        in_specs=placed,
        out_specs=(
            P(("gr", "tp"), "fs"),
            P("tp", None, "fs"),
            P("tp", None, "fs"),
            P("tp", None, "fs"),
        ),
        check_vma=False,
    )
```

```python
import jax
import jax.numpy as jnp
from jax import lax
from jax.experimental import pallas as pl
from jax.experimental.pallas import tpu as pltpu
from jax.sharding import PartitionSpec as P


norm_eps = 1e-06
BF = jnp.bfloat16
F32 = jnp.float32
CAP, TOK, D, F = 192, 512, 2048, 176
MAIN, REM = 128, 48
PACK_GU, PACK_D = 176, 88
PACK = PACK_GU + PACK_D
TRIPS = ((4, 5), (3, 7, 2, 6, 1, 0))
FAR = TRIPS[0] + TRIPS[1][:5]


def spec_vmem():
    return pl.BlockSpec(memory_space=pltpu.VMEM)


def call(body, outs, args, scratch=(), after=()):
    n, m = len(args), len(after)

    def run(*refs):
        body(*refs[:n], *refs[n + m :])

    return pl.pallas_call(
        run,
        out_shape=outs,
        in_specs=[pl.BlockSpec(memory_space=pltpu.SMEM)]
        + [spec_vmem()] * (n - 1)
        + [pl.BlockSpec(memory_space=pl.ANY)] * m,
        out_specs=jax.tree.map(lambda _: spec_vmem(), outs),
        scratch_shapes=list(scratch),
        compiler_params=pltpu.CompilerParams(vmem_limit_bytes=48 * 2**20),
    )(*args, *after)


def sds(*shape, dtype=BF):
    return jax.ShapeDtypeStruct(shape, dtype)


def peer(where, r):
    return ((where[0] + r // 2) % 4) * 2 + (where[1] + r % 2) % 2


def pack_body(where, gain, gate, up, down, *outs):
    g = gain[...]
    for r in range(8):
        e = peer(where, r)
        for top, mats in ((0, (gate[e] * g, up[e] * g)), (PACK_GU, (down[e],))):
            for h in range(2):
                pieces = []
                for m, mat in enumerate(mats):
                    at = top + 64 * m
                    outs[r // 2][r % 2, h, at : at + 64, :] = mat[:, h * F : h * F + MAIN].astype(BF)
                    rest = mat[:, h * F + MAIN : (h + 1) * F]
                    pieces += [rest[8 * i : 8 * i + 8] for i in range(8)]
                row = jnp.concatenate(pieces, axis=1)
                at = top + 64 * len(mats)
                rest = [row[:, 128 * i : 128 * i + 128] for i in range(row.shape[1] // 128)]
                outs[r // 2][r % 2, h, at : at + 8 * len(rest), :] = jnp.concatenate(
                    rest, axis=0
                ).astype(BF)


def swap_body(where, *refs):
    for dx in range(4):
        refs[4][dx] = refs[dx][1]


def by_y_body(where, *refs):
    got, swapped, outs, held = refs[:4], refs[4], refs[5:9], refs[9]
    for dx in range(4):
        held[2 * dx] = got[dx][0]
        held[2 * dx + 1] = swapped[dx]
    x, c, z, y = where[0], where[1], where[2], where[3]
    for dy in range(4):
        to_y = (y + dy) % 4
        for k in range(4):
            dx = (x + 8 - z - k) % 4
            r = dx * 2 + (c + to_y // 2) % 2
            outs[dy][k] = held[r, to_y % 2]


def by_z_body(where, *refs):
    got, out = refs[:4], refs[4]
    for z8 in range(8):
        k = (z8 + 4 - where[2]) % 4
        for j in range(4):
            out[z8, j] = got[j][k]


def unpack_body(where, got, *outs):
    z, y = where[2], where[3]

    @pl.loop(0, 8)
    def _(z8):
        for j in range(4):
            block = z8 * 4 + (y + 4 - j) % 4
            part = block // 2
            near = ((part // 4 + 4 - z) % 4) * 128 + (block % 2) * 64
            near = pl.multiple_of(near, 64)
            q = (part % 4 + 4 - y) % 4
            for top, mats in ((0, (0, 1)), (PACK_GU, (2,))):
                first, tiles = top + 64 * len(mats), 3 * len(mats)
                flat = got[z8, j, first : first + 8 * tiles, :].astype(F32)
                row = jnp.concatenate([flat[8 * i : 8 * i + 8] for i in range(tiles)], axis=1)
                for i, m in enumerate(mats):
                    main = got[z8, j, top + 64 * i : top + 64 * i + 64, :]
                    rest = jnp.concatenate(
                        [row[:, REM * p : REM * p + REM] for p in range(8 * i, 8 * i + 8)], axis=0
                    ).astype(BF)
                    outs[m][q, pl.ds(near, 64), 0:MAIN] = main
                    outs[m][q, pl.ds(near, 64), MAIN:F] = rest


def serve_body(where, *refs):
    z, y = where[2], where[3]
    for m in range(3):
        for q in range(4):
            for k in range(4):
                at = pl.multiple_of((((z + k) % 4) * 4 + (y + q) % 4) * 128, 128)
                refs[3 + m][0, pl.ds(at, 128), :] = refs[m][q, 128 * k : 128 * k + 128, :]


def dispatch_body(where, routes, *refs):
    toks, outs, near, table, made = refs[:4], refs[4:8], refs[8], refs[9], refs[10]
    expert = lax.broadcasted_iota(jnp.int32, (8, TOK), 0)
    named = (routes[0:1, :] == expert) | (routes[1:2, :] == expert)
    before = (
        lax.broadcasted_iota(jnp.int32, (TOK, TOK), 0)
        < lax.broadcasted_iota(jnp.int32, (TOK, TOK), 1)
    ).astype(F32).astype(BF)
    count = jnp.dot(named.astype(F32).astype(BF), before, preferred_element_type=F32)
    table[...] = jnp.where(named, count, -1.0)
    x = jnp.concatenate([t[...] for t in toks], axis=1)
    slot = lax.broadcasted_iota(jnp.int32, (CAP, TOK), 0).astype(F32)

    @pl.loop(0, 8)
    def _(r):
        pick = (slot == table[pl.ds(peer(where, r), 1), :]).astype(F32).astype(BF)
        made[r] = jnp.dot(pick, x, preferred_element_type=F32).astype(BF)

    near[...] = made[0]
    for r in range(8):
        outs[r // 2][r % 2] = made[r]


def rows_body(where, *refs):
    got, swapped, out = refs[:4], refs[4], refs[5]
    for i, r in enumerate(FAR):
        part = swapped[r // 2] if r % 2 else got[r // 2][0]
        out[CAP * i : CAP * i + CAP, :] = part


def first_ffn_body(where, *refs):
    ffn_of([x[...] for x in refs[:4]], *refs[4:])


def second_ffn_body(where, *refs):
    tiles, last, near, held = refs[:4], refs[4:8], refs[8:12], refs[-1]
    at_end = pl.program_id(0) == 2

    @pl.when(at_end)
    def _():
        for q in range(4):
            held[q, 0:CAP, :] = last[q][...]
            held[q, CAP : 2 * CAP, :] = near[q][...]

    @pl.when(jnp.logical_not(at_end))
    def _():
        for q in range(4):
            held[q] = tiles[q][...]

    ffn_of([held[q] for q in range(4)], *refs[12:-1])


def ffn_of(xs, wg, wu, wd, own, plus, minus, keep):
    g = u = total = None
    for q in range(4):
        x = xs[q]
        xf = x.astype(F32)
        dg = jnp.dot(x, wg[q], preferred_element_type=F32)
        du = jnp.dot(x, wu[q], preferred_element_type=F32)
        s = xf * xf
        g, u, total = (dg, du, s) if g is None else (g + dg, u + du, total + s)
    scale = lax.rsqrt(jnp.sum(total, axis=1, keepdims=True) / D + norm_eps)
    g = g * scale
    u = u * scale
    hidden = (g / (1.0 + jnp.exp(-g)) * u).astype(BF)

    def out(q, half):
        w = wd[q, 256 * half : 256 * half + 256, :]
        return lax.dot_general(
            hidden, w, (((1,), (1,)), ((), ())), preferred_element_type=F32
        ).astype(BF)

    plus[:, 0:256] = out(2, 0)
    plus[:, 256:512] = out(1, 1)
    minus[:, 0:256] = out(3, 0)
    minus[:, 256:512] = out(2, 1)
    keep[:, 0:256] = out(1, 0)
    keep[:, 256:512] = out(3, 1)
    own[:, 0:256] = out(0, 0)
    own[:, 256:512] = out(0, 1)


def ffn(t, where, rows, near, weights, after=()):
    tile, n = 2 * CAP, CAP * len(TRIPS[t])
    out = pl.BlockSpec((tile, 512), lambda i: (i, 0))
    if t == 0:
        body, tiled = first_ffn_body, rows
        specs = [out] * 4
    else:
        body, tiled = second_ffn_body, (*rows, *rows, *near)
        specs = [pl.BlockSpec((tile, 512), lambda i: (jnp.minimum(i, 1) + 1, 0))] * 4
        specs += [pl.BlockSpec((CAP, 512), lambda i: (6, 0))] * 4
        specs += [pl.BlockSpec((CAP, 512), lambda i: (0, 0))] * 4
    m = 1 + len(tiled) + len(weights)

    def run(*refs):
        body(*refs[:m], *refs[m + len(after) :])

    return pl.pallas_call(
        run,
        grid=(n // tile,),
        in_specs=[pl.BlockSpec(memory_space=pltpu.SMEM)]
        + specs
        + [pl.BlockSpec(a.shape, lambda i: (0, 0, 0)) for a in weights]
        + [pl.BlockSpec(memory_space=pl.ANY)] * len(after),
        out_specs=[out] * 4,
        out_shape=[sds(n, 512)] * 4,
        scratch_shapes=[pltpu.VMEM((4, tile, 512), BF)] if t else [],
        compiler_params=pltpu.CompilerParams(vmem_limit_bytes=48 * 2**20),
    )(where, *tiled, *weights, *after)


def add_body(where, keep, from_left, from_right, out0, out1):
    out0[...] = (keep[:, 0:256].astype(F32) + from_left[:, 0:256].astype(F32)).astype(BF)
    out1[...] = (keep[:, 256:512].astype(F32) + from_right[:, 256:512].astype(F32)).astype(BF)


def sums_body(where, own, from_left, from_right, left, right, *outs):
    for i, out in enumerate(outs):
        at = slice(CAP * i, CAP * i + CAP)
        a = own[at, 0:256].astype(F32) + left[at, :].astype(F32)
        out[:, 0:256] = (a + from_right[at, 0:256].astype(F32)).astype(BF)
        b = own[at, 256:512].astype(F32) + right[at, :].astype(F32)
        out[:, 256:512] = (b + from_left[at, 256:512].astype(F32)).astype(BF)


def plan_body(where, routes, weight, out):
    expert = lax.broadcasted_iota(jnp.int32, (TOK, 128), 1)
    named = (routes[:, 0:1] == expert) | (routes[:, 1:2] == expert)
    named = named.astype(F32).astype(BF)
    lane = lax.broadcasted_iota(jnp.int32, (128, 128), 1)

    @pl.loop(0, 4)
    def _(t):
        at = pl.ds(pl.multiple_of(t * 128, 128), 128)
        r0, r1 = routes[at, 0:1], routes[at, 1:2]
        w0, w1 = weight[at, 0:1], weight[at, 1:2]
        before = (
            lax.broadcasted_iota(jnp.int32, (128, TOK), 1)
            < lax.broadcasted_iota(jnp.int32, (128, TOK), 0) + t * 128
        ).astype(F32).astype(BF)
        count = jnp.dot(before, named, preferred_element_type=F32)
        slot0 = jnp.sum(jnp.where(r0 == lane, count, 0.0), axis=1, keepdims=True)
        slot1 = jnp.sum(jnp.where(r1 == lane, count, 0.0), axis=1, keepdims=True)
        table = jnp.zeros((128, 128), F32)
        for r in range(8):
            e = peer(where, r)
            slot = jnp.where(r0 == e, slot0, jnp.where(r1 == e, slot1, -1.0))
            w = jnp.where(r0 == e, w0, jnp.where(r1 == e, w1, 0.0))
            table = jnp.where(lane == r, slot, jnp.where(lane == 8 + r, w, table))
        out[at, :] = table


def combine_body(relative, plan, *refs):
    n = len(relative)
    got, outs = refs[:n], refs[n:]
    slot = lax.broadcasted_iota(jnp.int32, (TOK, CAP), 1).astype(F32)
    total = None
    if len(outs) == 5:
        total, outs = outs[0][...], outs[1:]
    for i, r in enumerate(relative):
        pick = (slot == plan[:, r : r + 1]).astype(F32).astype(BF)
        part = plan[:, 8 + r : 9 + r] * jnp.dot(pick, got[i][...], preferred_element_type=F32)
        total = part if total is None else total + part
    if len(outs) == 1:
        outs[0][...] = total
        return
    outs[0][...] = total[:, 0:128]
    for k in range(1, 4):
        outs[k][...] = total[:, 128 * k : 128 * k + 128].astype(BF)


def shift_tp(a, r, sign=1):
    dx, dc = sign * (r // 2), r % 2
    return lax.ppermute(
        a, "tp", [(2 * x + c, 2 * ((x + dx) % 4) + (c + dc) % 2) for x in range(4) for c in range(2)]
    )


def shift_fs(a, dz, dy):
    return lax.ppermute(
        a, "fs", [(4 * z + y, 4 * ((z + dz) % 4) + (y + dy) % 4) for z in range(4) for y in range(4)]
    )


def local(tokens, routes, route_weight, norm_gain, gate_master, up_master, down_master):
    tp, fs, gr = lax.axis_index("tp"), lax.axis_index("fs"), lax.axis_index("gr")
    where = jnp.stack([tp // 2, tp % 2, fs // 4, fs % 4, gr]).astype(jnp.int32)
    by_k = [tokens] * 4
    for k in (2, 1, 3):
        by_k[k] = shift_fs(tokens, -k, 0)
    packed = call(
        pack_body,
        [sds(2, 2, PACK, 128)] * 4,
        (where, norm_gain[:, None], gate_master, up_master, down_master),
    )

    def over_x(parts):
        out = list(parts)
        for dx in (2, 1, 3):
            out[dx] = shift_tp(parts[dx], 2 * dx)
        return out

    def swap(parts, after):
        shape = (4, *parts[0].shape[1:])
        mine = call(swap_body, [sds(*shape)], (where, *parts), after=after)[0]
        return mine, shift_tp(mine, 1)

    w_x = over_x(packed)
    *slots, near = call(
        dispatch_body,
        [sds(2, CAP, 512)] * 4 + [sds(CAP, 512)],
        (where, routes.T, *by_k),
        scratch=[pltpu.VMEM((8, TOK), F32), pltpu.VMEM((8, CAP, 512), BF)],
        after=(packed[0],),
    )
    t_x = over_x(slots)

    def over_y(own):
        two, plus, minus = shift_fs(own, 0, 2), shift_fs(own, 0, 1), shift_fs(own, 0, -1)
        return own, minus, two, plus

    near = over_y(near)
    _, w_core = swap(w_x, (slots[0],))

    to_y = call(
        by_y_body,
        [sds(4, PACK, 128)] * 4,
        (where, *w_x, w_core),
        scratch=[pltpu.VMEM((8, 2, PACK, 128), BF)],
    )
    w_y = list(to_y)
    for dy in (2, 1, 3):
        w_y[dy] = shift_fs(to_y[dy], 0, dy)
    plan = call(
        plan_body, [sds(TOK, 128, dtype=F32)], (where, routes, route_weight), after=(to_y[0],)
    )[0]
    _, t_core = swap(t_x, (plan,))
    own = call(rows_body, [sds(CAP * len(FAR), 512)], (where, *t_x, t_core))[0]
    rows = over_y(own)
    to_z = call(by_z_body, [sds(8, 4, PACK, 128)], (where, *w_y), after=(own,))[0]
    w_z = lax.all_to_all(
        to_z,
        ("gr", "fs"),
        0,
        0,
        axis_index_groups=[[4 * z + y for z in range(8)] for y in range(4)],
        tiled=True,
    )
    ordered = call(unpack_body, [sds(4, 512, F)] * 3, (where, w_z))
    made = [ffn(0, where, rows, near, ordered)]
    made.append(ffn(1, where, rows, near, ordered, (made[0][0],)))

    def out_y(t):
        return shift_fs(made[t][1], 0, 1), shift_fs(made[t][2], 0, -1)

    def sum_y(t, got, after):
        n = CAP * len(TRIPS[t])
        sums = call(add_body, [sds(n, 256)] * 2, (where, made[t][3], *got), after=after)
        return sums[0], (shift_fs(sums[0], 0, 1), shift_fs(sums[1], 0, -1))

    def home(t, got, ends, after):
        places = TRIPS[t]
        sums = call(
            sums_body, [sds(CAP, 512)] * len(places), (where, made[t][0], *got, *ends), after=after
        )
        return sums[0], [p if r == 0 else shift_tp(p, r, -1) for r, p in zip(places, sums)]

    def combine(t, parts, outs, after=()):
        return call(
            lambda where, plan, *refs: combine_body(TRIPS[t], plan, *refs),
            outs,
            (where, plan, *parts),
            after=after,
        )

    got = [out_y(t) for t in range(2)]
    add0, ends0 = sum_y(0, got[0], (made[1][0],))
    gate_w, up_w, down_w = call(serve_body, [sds(1, D, F)] * 3, (where, *ordered), after=(add0,))
    add1, ends1 = sum_y(1, got[1], (gate_w,))
    sums0, home0 = home(0, got[0], ends0, (add1,))
    sums1, home1 = home(1, got[1], ends1, (sums0,))
    part = combine(0, home0, [sds(TOK, 512, dtype=F32)], (sums1,))
    mixed = combine(1, (*home1, *part), [sds(TOK, 128, dtype=F32)] + [sds(TOK, 128)] * 3)
    out = mixed[0]
    for k in (2, 1, 3):
        got = shift_fs(mixed[k], k, 0)
        out = out + got.astype(F32)
    return (out.astype(BF), gate_w, up_w, down_w)


def solution(mesh):
    placed = (
        P(("gr", "tp"), "fs"),
        P(("gr", "tp"), None),
        P(("gr", "tp"), None),
        P(("gr", "fs")),
        P(None, ("gr", "fs"), "tp"),
        P(None, ("gr", "fs"), "tp"),
        P(None, ("gr", "fs"), "tp"),
    )

    return jax.shard_map(
        local,
        mesh=mesh,
        in_specs=placed,
        out_specs=(
            P(("gr", "tp"), "fs"),
            P("tp", None, "fs"),
            P("tp", None, "fs"),
            P("tp", None, "fs"),
        ),
        check_vma=False,
    )
```

```python
import jax
import jax.numpy as jnp
from jax import lax
from jax.experimental import pallas as pl
from jax.experimental.pallas import tpu as pltpu
from jax.sharding import PartitionSpec as P


norm_eps = 1e-06
BF = jnp.bfloat16
F32 = jnp.float32
CAP, TOK, D, F = 192, 512, 2048, 176
MAIN, REM = 128, 48
PACK_GU, PACK_D = 176, 88
PACK = PACK_GU + PACK_D
TRIPS = ((4, 5), (3, 7, 2, 6, 1, 0))
FAR = TRIPS[0] + TRIPS[1][:5]


def spec_vmem():
    return pl.BlockSpec(memory_space=pltpu.VMEM)


def call(body, outs, args, scratch=(), after=()):
    n, m = len(args), len(after)

    def run(*refs):
        body(*refs[:n], *refs[n + m :])

    return pl.pallas_call(
        run,
        out_shape=outs,
        in_specs=[pl.BlockSpec(memory_space=pltpu.SMEM)]
        + [spec_vmem()] * (n - 1)
        + [pl.BlockSpec(memory_space=pl.ANY)] * m,
        out_specs=jax.tree.map(lambda _: spec_vmem(), outs),
        scratch_shapes=list(scratch),
        compiler_params=pltpu.CompilerParams(vmem_limit_bytes=48 * 2**20),
    )(*args, *after)


def sds(*shape, dtype=BF):
    return jax.ShapeDtypeStruct(shape, dtype)


def peer(where, r):
    return ((where[0] + r // 2) % 4) * 2 + (where[1] + r % 2) % 2


def pack_body(where, gain, gate, up, down, *outs):
    row = lax.broadcasted_iota(jnp.int32, (64, 64), 0)
    col = lax.broadcasted_iota(jnp.int32, (64, 64), 1)
    g = jnp.sum(jnp.where(row == col, gain[...], 0.0), axis=1, keepdims=True)
    for r in range(8):
        e = peer(where, r)
        for top, mats in ((0, (gate[e] * g, up[e] * g)), (PACK_GU, (down[e],))):
            for h in range(2):
                pieces = []
                for m, mat in enumerate(mats):
                    at = top + 64 * m
                    outs[r // 2][r % 2, h, at : at + 64, :] = mat[:, h * F : h * F + MAIN].astype(BF)
                    rest = mat[:, h * F + MAIN : (h + 1) * F]
                    pieces += [rest[8 * i : 8 * i + 8] for i in range(8)]
                row = jnp.concatenate(pieces, axis=1)
                at = top + 64 * len(mats)
                rest = [row[:, 128 * i : 128 * i + 128] for i in range(row.shape[1] // 128)]
                outs[r // 2][r % 2, h, at : at + 8 * len(rest), :] = jnp.concatenate(
                    rest, axis=0
                ).astype(BF)


def swap_body(where, *refs):
    for dx in range(4):
        refs[4][dx] = refs[dx][1]


def by_y_body(where, *refs):
    got, swapped, outs, held = refs[:4], refs[4], refs[5:9], refs[9]
    for dx in range(4):
        held[2 * dx] = got[dx][0]
        held[2 * dx + 1] = swapped[dx]
    x, c, z, y = where[0], where[1], where[2], where[3]
    for dy in range(4):
        to_y = (y + dy) % 4
        for k in range(4):
            dx = (x + 8 - z - k) % 4
            r = dx * 2 + (c + to_y // 2) % 2
            outs[dy][k] = held[r, to_y % 2]


def by_z_body(where, *refs):
    got, out = refs[:4], refs[4]
    for z8 in range(8):
        k = (z8 + 4 - where[2]) % 4
        for j in range(4):
            out[z8, j] = got[j][k]


def unpack_body(where, got, *outs):
    z, y = where[2], where[3]

    @pl.loop(0, 8)
    def _(z8):
        for j in range(4):
            block = z8 * 4 + (y + 4 - j) % 4
            part = block // 2
            near = ((part // 4 + 4 - z) % 4) * 128 + (block % 2) * 64
            near = pl.multiple_of(near, 64)
            q = (part % 4 + 4 - y) % 4
            for top, mats in ((0, (0, 1)), (PACK_GU, (2,))):
                first, tiles = top + 64 * len(mats), 3 * len(mats)
                flat = got[z8, j, first : first + 8 * tiles, :].astype(F32)
                row = jnp.concatenate([flat[8 * i : 8 * i + 8] for i in range(tiles)], axis=1)
                for i, m in enumerate(mats):
                    main = got[z8, j, top + 64 * i : top + 64 * i + 64, :]
                    rest = jnp.concatenate(
                        [row[:, REM * p : REM * p + REM] for p in range(8 * i, 8 * i + 8)], axis=0
                    ).astype(BF)
                    outs[m][q, pl.ds(near, 64), 0:MAIN] = main
                    outs[m][q, pl.ds(near, 64), MAIN:F] = rest


def serve_body(where, *refs):
    z, y = where[2], where[3]
    for m in range(3):
        for q in range(4):
            for k in range(4):
                at = pl.multiple_of((((z + k) % 4) * 4 + (y + q) % 4) * 128, 128)
                refs[3 + m][0, pl.ds(at, 128), :] = refs[m][q, 128 * k : 128 * k + 128, :]


def dispatch_body(where, routes, *refs):
    toks, outs, near, table, made = refs[:4], refs[4:8], refs[8], refs[9], refs[10]
    expert = lax.broadcasted_iota(jnp.int32, (8, TOK), 0)
    named = (routes[0:1, :] == expert) | (routes[1:2, :] == expert)
    before = (
        lax.broadcasted_iota(jnp.int32, (TOK, TOK), 0)
        < lax.broadcasted_iota(jnp.int32, (TOK, TOK), 1)
    ).astype(F32).astype(BF)
    count = jnp.dot(named.astype(F32).astype(BF), before, preferred_element_type=F32)
    table[...] = jnp.where(named, count, -1.0)
    x = jnp.concatenate([t[...] for t in toks], axis=1)
    slot = lax.broadcasted_iota(jnp.int32, (CAP, TOK), 0).astype(F32)

    @pl.loop(0, 8)
    def _(r):
        pick = (slot == table[pl.ds(peer(where, r), 1), :]).astype(F32).astype(BF)
        made[r] = jnp.dot(pick, x, preferred_element_type=F32).astype(BF)

    near[...] = made[0]
    for r in range(8):
        outs[r // 2][r % 2] = made[r]


def rows_body(where, *refs):
    got, swapped, out = refs[:4], refs[4], refs[5]
    for i, r in enumerate(FAR):
        part = swapped[r // 2] if r % 2 else got[r // 2][0]
        out[CAP * i : CAP * i + CAP, :] = part


def first_ffn_body(where, *refs):
    ffn_of([x[...] for x in refs[:4]], *refs[4:])


def second_ffn_body(where, *refs):
    tiles, last, near, held = refs[:4], refs[4:8], refs[8:12], refs[-1]
    at_end = pl.program_id(0) == 2

    @pl.when(at_end)
    def _():
        for q in range(4):
            held[q, 0:CAP, :] = last[q][...]
            held[q, CAP : 2 * CAP, :] = near[q][...]

    @pl.when(jnp.logical_not(at_end))
    def _():
        for q in range(4):
            held[q] = tiles[q][...]

    ffn_of([held[q] for q in range(4)], *refs[12:-1])


def ffn_of(xs, wg, wu, wd, own, plus, minus, keep):
    g = u = total = None
    for q in range(4):
        x = xs[q]
        xf = x.astype(F32)
        dg = jnp.dot(x, wg[q], preferred_element_type=F32)
        du = jnp.dot(x, wu[q], preferred_element_type=F32)
        s = xf * xf
        g, u, total = (dg, du, s) if g is None else (g + dg, u + du, total + s)
    scale = lax.rsqrt(jnp.sum(total, axis=1, keepdims=True) / D + norm_eps)
    g = g * scale
    u = u * scale
    hidden = (g / (1.0 + jnp.exp(-g)) * u).astype(BF)

    def out(q, half):
        w = wd[q, 256 * half : 256 * half + 256, :]
        return lax.dot_general(
            hidden, w, (((1,), (1,)), ((), ())), preferred_element_type=F32
        ).astype(BF)

    plus[:, 0:256] = out(2, 0)
    plus[:, 256:512] = out(1, 1)
    minus[:, 0:256] = out(3, 0)
    minus[:, 256:512] = out(2, 1)
    keep[:, 0:256] = out(1, 0)
    keep[:, 256:512] = out(3, 1)
    own[:, 0:256] = out(0, 0)
    own[:, 256:512] = out(0, 1)


def ffn(t, where, rows, near, weights, after=()):
    tile, n = 2 * CAP, CAP * len(TRIPS[t])
    out = pl.BlockSpec((tile, 512), lambda i: (i, 0))
    if t == 0:
        body, tiled = first_ffn_body, rows
        specs = [out] * 4
    else:
        body, tiled = second_ffn_body, (*rows, *rows, *near)
        specs = [pl.BlockSpec((tile, 512), lambda i: (jnp.minimum(i, 1) + 1, 0))] * 4
        specs += [pl.BlockSpec((CAP, 512), lambda i: (6, 0))] * 4
        specs += [pl.BlockSpec((CAP, 512), lambda i: (0, 0))] * 4
    m = 1 + len(tiled) + len(weights)

    def run(*refs):
        body(*refs[:m], *refs[m + len(after) :])

    return pl.pallas_call(
        run,
        grid=(n // tile,),
        in_specs=[pl.BlockSpec(memory_space=pltpu.SMEM)]
        + specs
        + [pl.BlockSpec(a.shape, lambda i: (0, 0, 0)) for a in weights]
        + [pl.BlockSpec(memory_space=pl.ANY)] * len(after),
        out_specs=[out] * 4,
        out_shape=[sds(n, 512)] * 4,
        scratch_shapes=[pltpu.VMEM((4, tile, 512), BF)] if t else [],
        compiler_params=pltpu.CompilerParams(vmem_limit_bytes=48 * 2**20),
    )(where, *tiled, *weights, *after)


def add_body(where, keep, from_left, from_right, out0, out1):
    out0[...] = (keep[:, 0:256].astype(F32) + from_left[:, 0:256].astype(F32)).astype(BF)
    out1[...] = (keep[:, 256:512].astype(F32) + from_right[:, 256:512].astype(F32)).astype(BF)


def sums_body(where, own, from_left, from_right, left, right, *outs):
    for i, out in enumerate(outs):
        at = slice(CAP * i, CAP * i + CAP)
        a = own[at, 0:256].astype(F32) + left[at, :].astype(F32)
        out[:, 0:256] = (a + from_right[at, 0:256].astype(F32)).astype(BF)
        b = own[at, 256:512].astype(F32) + right[at, :].astype(F32)
        out[:, 256:512] = (b + from_left[at, 256:512].astype(F32)).astype(BF)


def plan_body(where, routes, weight, out):
    expert = lax.broadcasted_iota(jnp.int32, (TOK, 128), 1)
    named = (routes[:, 0:1] == expert) | (routes[:, 1:2] == expert)
    named = named.astype(F32).astype(BF)
    lane = lax.broadcasted_iota(jnp.int32, (128, 128), 1)

    @pl.loop(0, 4)
    def _(t):
        at = pl.ds(pl.multiple_of(t * 128, 128), 128)
        r0, r1 = routes[at, 0:1], routes[at, 1:2]
        w0, w1 = weight[at, 0:1], weight[at, 1:2]
        before = (
            lax.broadcasted_iota(jnp.int32, (128, TOK), 1)
            < lax.broadcasted_iota(jnp.int32, (128, TOK), 0) + t * 128
        ).astype(F32).astype(BF)
        count = jnp.dot(before, named, preferred_element_type=F32)
        slot0 = jnp.sum(jnp.where(r0 == lane, count, 0.0), axis=1, keepdims=True)
        slot1 = jnp.sum(jnp.where(r1 == lane, count, 0.0), axis=1, keepdims=True)
        table = jnp.zeros((128, 128), F32)
        for r in range(8):
            e = peer(where, r)
            slot = jnp.where(r0 == e, slot0, jnp.where(r1 == e, slot1, -1.0))
            w = jnp.where(r0 == e, w0, jnp.where(r1 == e, w1, 0.0))
            table = jnp.where(lane == r, slot, jnp.where(lane == 8 + r, w, table))
        out[at, :] = table


def combine_body(relative, plan, *refs):
    n = len(relative)
    got, outs = refs[:n], refs[n:]
    slot = lax.broadcasted_iota(jnp.int32, (TOK, CAP), 1).astype(F32)
    total = None
    if len(outs) == 5:
        total, outs = outs[0][...], outs[1:]
    for i, r in enumerate(relative):
        pick = (slot == plan[:, r : r + 1]).astype(F32).astype(BF)
        part = plan[:, 8 + r : 9 + r] * jnp.dot(pick, got[i][...], preferred_element_type=F32)
        total = part if total is None else total + part
    if len(outs) == 1:
        outs[0][...] = total
        return
    outs[0][...] = total[:, 0:128]
    for k in range(1, 4):
        outs[k][...] = total[:, 128 * k : 128 * k + 128].astype(BF)


def shift_tp(a, r, sign=1):
    dx, dc = sign * (r // 2), r % 2
    return lax.ppermute(
        a, "tp", [(2 * x + c, 2 * ((x + dx) % 4) + (c + dc) % 2) for x in range(4) for c in range(2)]
    )


def shift_fs(a, dz, dy):
    return lax.ppermute(
        a, "fs", [(4 * z + y, 4 * ((z + dz) % 4) + (y + dy) % 4) for z in range(4) for y in range(4)]
    )


def local(tokens, routes, route_weight, norm_gain, gate_master, up_master, down_master):
    tp, fs, gr = lax.axis_index("tp"), lax.axis_index("fs"), lax.axis_index("gr")
    where = jnp.stack([tp // 2, tp % 2, fs // 4, fs % 4, gr]).astype(jnp.int32)
    by_k = [tokens] * 4
    for k in (2, 1, 3):
        by_k[k] = shift_fs(tokens, -k, 0)
    packed = call(
        pack_body,
        [sds(2, 2, PACK, 128)] * 4,
        (where, norm_gain[None, :], gate_master, up_master, down_master),
    )

    def over_x(parts):
        out = list(parts)
        for dx in (2, 1, 3):
            out[dx] = shift_tp(parts[dx], 2 * dx)
        return out

    def swap(parts, after):
        shape = (4, *parts[0].shape[1:])
        mine = call(swap_body, [sds(*shape)], (where, *parts), after=after)[0]
        return mine, shift_tp(mine, 1)

    w_x = over_x(packed)
    *slots, near = call(
        dispatch_body,
        [sds(2, CAP, 512)] * 4 + [sds(CAP, 512)],
        (where, routes.T, *by_k),
        scratch=[pltpu.VMEM((8, TOK), F32), pltpu.VMEM((8, CAP, 512), BF)],
        after=(packed[0],),
    )
    t_x = over_x(slots)

    def over_y(own):
        two, plus, minus = shift_fs(own, 0, 2), shift_fs(own, 0, 1), shift_fs(own, 0, -1)
        return own, minus, two, plus

    near = over_y(near)
    _, w_core = swap(w_x, (slots[0],))

    to_y = call(
        by_y_body,
        [sds(4, PACK, 128)] * 4,
        (where, *w_x, w_core),
        scratch=[pltpu.VMEM((8, 2, PACK, 128), BF)],
    )
    w_y = list(to_y)
    for dy in (2, 1, 3):
        w_y[dy] = shift_fs(to_y[dy], 0, dy)
    plan = call(
        plan_body, [sds(TOK, 128, dtype=F32)], (where, routes, route_weight), after=(to_y[0],)
    )[0]
    _, t_core = swap(t_x, (plan,))
    own = call(rows_body, [sds(CAP * len(FAR), 512)], (where, *t_x, t_core))[0]
    rows = over_y(own)
    to_z = call(by_z_body, [sds(8, 4, PACK, 128)], (where, *w_y), after=(own,))[0]
    w_z = lax.all_to_all(
        to_z,
        ("gr", "fs"),
        0,
        0,
        axis_index_groups=[[4 * z + y for z in range(8)] for y in range(4)],
        tiled=True,
    )
    ordered = call(unpack_body, [sds(4, 512, F)] * 3, (where, w_z))
    made = [ffn(0, where, rows, near, ordered)]
    made.append(ffn(1, where, rows, near, ordered, (made[0][0],)))

    def out_y(t):
        return shift_fs(made[t][1], 0, 1), shift_fs(made[t][2], 0, -1)

    def sum_y(t, got, after):
        n = CAP * len(TRIPS[t])
        sums = call(add_body, [sds(n, 256)] * 2, (where, made[t][3], *got), after=after)
        return sums[0], (shift_fs(sums[0], 0, 1), shift_fs(sums[1], 0, -1))

    def home(t, got, ends, after):
        places = TRIPS[t]
        sums = call(
            sums_body, [sds(CAP, 512)] * len(places), (where, made[t][0], *got, *ends), after=after
        )
        return sums[0], [p if r == 0 else shift_tp(p, r, -1) for r, p in zip(places, sums)]

    def combine(t, parts, outs, after=()):
        return call(
            lambda where, plan, *refs: combine_body(TRIPS[t], plan, *refs),
            outs,
            (where, plan, *parts),
            after=after,
        )

    got = [out_y(t) for t in range(2)]
    add0, ends0 = sum_y(0, got[0], (made[1][0],))
    gate_w, up_w, down_w = call(serve_body, [sds(1, D, F)] * 3, (where, *ordered), after=(add0,))
    add1, ends1 = sum_y(1, got[1], (gate_w,))
    sums0, home0 = home(0, got[0], ends0, (add1,))
    sums1, home1 = home(1, got[1], ends1, (sums0,))
    part = combine(0, home0, [sds(TOK, 512, dtype=F32)], (sums1,))
    mixed = combine(1, (*home1, *part), [sds(TOK, 128, dtype=F32)] + [sds(TOK, 128)] * 3)
    out = mixed[0]
    for k in (2, 1, 3):
        got = shift_fs(mixed[k], k, 0)
        out = out + got.astype(F32)
    return (out.astype(BF), gate_w, up_w, down_w)


def solution(mesh):
    placed = (
        P(("gr", "tp"), "fs"),
        P(("gr", "tp"), None),
        P(("gr", "tp"), None),
        P(("gr", "fs")),
        P(None, ("gr", "fs"), "tp"),
        P(None, ("gr", "fs"), "tp"),
        P(None, ("gr", "fs"), "tp"),
    )

    return jax.shard_map(
        local,
        mesh=mesh,
        in_specs=placed,
        out_specs=(
            P(("gr", "tp"), "fs"),
            P("tp", None, "fs"),
            P("tp", None, "fs"),
            P("tp", None, "fs"),
        ),
        check_vma=False,
    )
```
